512 devices in a mesh: sp: 128 (over z, y, core), tp: 4 (over x).
Axes of the slice: x: 4, y: 8, z: 8, core: 2. Of those that a mesh axis runs over, the one named last changes fastest.
Arguments:
- tokens: bfloat16 [65536, 2048], P('sp', 'tp'), may hold values from -6 to 6
- norm_gain: float32 [2048], replicated, may hold values from 0.1 to 1.9
- query_weight: bfloat16 [2048, 2048], P('sp', 'tp'), may hold values from -0.125 to 0.125
- key_weight: bfloat16 [2048, 512], P('sp', 'tp'), may hold values from -0.125 to 0.125
- value_weight: bfloat16 [2048, 512], P('sp', 'tp'), may hold values from -0.125 to 0.125
- pool_in_weight: bfloat16 [2048, 1024], P('sp', 'tp'), may hold values from -0.125 to 0.125
- pool_mix_weight: bfloat16 [4, 256, 256], P('tp'), may hold values from -0.375 to 0.375
- sink_logit: float32 [32], P('tp'), may hold values from -300 to 300
- out_pool_weight: bfloat16 [1024, 2048], P('tp', 'sp'), may hold values from -0.109375 to 0.109375
- out_attn_weight: bfloat16 [2048, 2048], P('tp', 'sp'), may hold values from -1.25 to 1.25
Outputs:
- mixed: bfloat16 [65536, 2048], P('sp', 'tp')
- log_weight: float32 [32, 65536], P('tp', 'sp')
The draws below stay inside these ranges and needn't reach their ends.
All inputs are finite; a program needn't handle non-finite values.
Results may differ from the reference program's by a relative error of at most 0.012.
Values may be sent and summed in bfloat16 or wider, within the bound.
A program may use at most 64 MiB of HBM per device.

```python
import jax
import jax.numpy as jnp
from jax import lax

D = 2048
HQ = 32
KVH = 8
HD = 64
GROUPS = 4
POOL_GC = 256
WINDOW = 128
GRID_W = 64
POOL_WIDTH = 1024
TOKENS = 65536
N_TP = 4


def draw_sink_logit(key, part):
    heads_per_group = HQ // KVH
    drawn = jax.random.uniform(jax.random.fold_in(key, 11), (KVH, heads_per_group), jnp.float32, 2.0, 6.0)
    return drawn.reshape(HQ)


def block_scale(key, shape, cuts, low, largest):
    gain, own = 1.0, jax.random.fold_in(key, 6)
    for position, parts in cuts:
        heights = jnp.exp(jax.random.uniform(jax.random.fold_in(own, position), (parts,), jnp.float32, low / len(cuts), largest / len(cuts)))
        gain = gain * jnp.repeat(heights, shape[position] // parts).reshape([-1 if axis == position else 1 for axis in range(len(shape))])
    return gain


def scatter_about(stream_key, dims, spread, bound, pieces=(), kind=jnp.bfloat16):
    values = jax.random.normal(stream_key, dims, jnp.float32) * spread
    if len(pieces) > 0:
        values = block_scale(stream_key, dims, pieces, -0.22, 0.18) * values
    return jnp.clip(values, min=-bound, max=bound).astype(kind)


def setup_inputs(seed: int = 0) -> dict:
    streams_of = jax.random.split(jax.random.key(seed), 11)
    tokens = scatter_about(streams_of[0], (TOKENS, D), 1.0, 6.0, ((0, 128), (1, 4)))
    norm_gain = jnp.clip(1.0 + 0.18 * jax.random.normal(streams_of[1], (D,), jnp.float32), 0.1, 1.9)
    query_weight = scatter_about(streams_of[2], (D, HQ * HD), D ** -0.5, 0.125, ((0, 128), (1, 4)))
    key_weight = scatter_about(streams_of[3], (D, KVH * HD), D ** -0.5, 0.125, ((0, 128), (1, 4)))
    value_weight = scatter_about(streams_of[4], (D, KVH * HD), D ** -0.5, 0.125, ((0, 128), (1, 4)))
    pool_in_weight = scatter_about(streams_of[5], (D, POOL_WIDTH), D ** -0.5, 0.125, ((0, 128), (1, 4)))
    pool_mix_weight = scatter_about(streams_of[6], (GROUPS, POOL_GC, POOL_GC), POOL_GC ** -0.5, 0.375, ((0, 4),))
    sink_logit = draw_sink_logit(jax.random.fold_in(streams_of[10], 71), 0)
    out_pool_weight = scatter_about(streams_of[8], (POOL_WIDTH, D), (POOL_WIDTH + HQ * HD) ** -0.5, 0.109375, ((0, 4), (1, 128)))
    out_attn_weight = scatter_about(streams_of[9], (HQ * HD, D), ((POOL_WIDTH + HQ * HD) // 144) ** -0.5, 1.25, ((0, 4), (1, 128)))
    return {"tokens": tokens, "norm_gain": norm_gain, "query_weight": query_weight, "key_weight": key_weight, "value_weight": value_weight, "pool_in_weight": pool_in_weight, "pool_mix_weight": pool_mix_weight, "sink_logit": sink_logit, "out_pool_weight": out_pool_weight, "out_attn_weight": out_attn_weight}


norm_eps = 1e-06
rope_base = 10000.0
pool_reach = 8
neg_fill = -1e+30

def rope_tables(positions, head_dim):
    n_freq = head_dim // 4
    freqs = rope_base ** (-jnp.arange(n_freq, dtype=jnp.float32) / n_freq)
    rows = (positions // GRID_W).astype(jnp.float32)
    columns = (positions % GRID_W).astype(jnp.float32)
    row_angle = rows[:, None] * freqs[None, :]
    col_angle = columns[:, None] * freqs[None, :]
    return (jnp.cos(row_angle), jnp.sin(row_angle), jnp.cos(col_angle), jnp.sin(col_angle))

def rotate_half(values, cosine, sine):
    middle = values.shape[-1] // 2
    first = values[..., :middle]
    second = values[..., middle:]
    return jnp.concatenate([first * cosine - second * sine, second * cosine + first * sine], -1)

def rotate_heads(values, tables, head_dim):
    rows_count = values.shape[0]
    shaped = values.astype(jnp.float32).reshape(rows_count, -1, head_dim)
    cos_r, sin_r, cos_c, sin_c = [table[:, None, :] for table in tables]
    split = head_dim // 2
    turned = jnp.concatenate([rotate_half(shaped[..., :split], cos_r, sin_r), rotate_half(shaped[..., split:], cos_c, sin_c)], -1)
    return turned.reshape(rows_count, -1).astype(jnp.bfloat16)

def pool_group(extended, own, positions, half_width, seq_total):
    rows_count = own.shape[0]
    summed = jnp.zeros(own.shape, jnp.float32)
    counted = jnp.zeros((rows_count,), jnp.float32)
    for shift_by in range(-pool_reach, pool_reach):
        source = positions + shift_by
        inside = (shift_by >= -half_width) & (shift_by < half_width) & (source >= 0) & (source < seq_total)
        window_rows = extended[pool_reach + shift_by:pool_reach + shift_by + rows_count].astype(jnp.float32)
        summed = summed + jnp.where(inside[:, None], window_rows, 0.0)
        counted = counted + inside.astype(jnp.float32)
    return (summed / counted[:, None] - own.astype(jnp.float32)).astype(jnp.bfloat16)

def attend_block(queries, keys, values, sink, query_pos, key_pos, seq_total):
    scores = jnp.einsum('qhgd,khd->hgqk', queries.astype(jnp.float32), keys.astype(jnp.float32)) * HD ** (-0.5)
    valid = (jnp.abs(query_pos[:, None] - key_pos[None, :]) <= WINDOW) & (key_pos >= 0)[None, :] & (key_pos < seq_total)[None, :]
    scores = jnp.where(valid, scores, neg_fill)
    row_top = jnp.maximum(lax.optimization_barrier(jnp.max(scores, -1)), sink[:, :, None])
    exps = jnp.exp(scores - row_top[..., None])
    row_total = lax.optimization_barrier(jnp.sum(exps, -1)) + jnp.exp(sink[:, :, None] - row_top)
    weights = (exps / row_total[..., None]).astype(jnp.bfloat16)
    attended = jnp.einsum('hgqk,khd->qhgd', weights.astype(jnp.float32), values.astype(jnp.float32))
    return (attended.astype(jnp.bfloat16), row_top + jnp.log(row_total))

def reference(tokens, norm_gain, query_weight, key_weight, value_weight, pool_in_weight, pool_mix_weight, sink_logit, out_pool_weight, out_attn_weight):
    seq_total = tokens.shape[0]
    wide = tokens.astype(jnp.float32)
    normed = (wide * lax.rsqrt(lax.optimization_barrier(jnp.mean(wide * wide, -1, keepdims=True)) + norm_eps) * norm_gain).astype(jnp.bfloat16)
    query = jnp.dot(normed, query_weight, preferred_element_type=jnp.float32).astype(jnp.bfloat16)
    key = jnp.dot(normed, key_weight, preferred_element_type=jnp.float32).astype(jnp.bfloat16)
    value = jnp.dot(normed, value_weight, preferred_element_type=jnp.float32).astype(jnp.bfloat16)
    pool_input = jnp.dot(normed, pool_in_weight, preferred_element_type=jnp.float32).astype(jnp.bfloat16)
    positions = jnp.arange(seq_total, dtype=jnp.int32)
    tables = rope_tables(positions, HD)
    rot_query = rotate_heads(query, tables, HD)
    rot_key = rotate_heads(key, tables, HD)
    pool_parts = []
    for group in range(GROUPS):
        own = pool_input[:, group * POOL_GC:(group + 1) * POOL_GC]
        extended = jnp.pad(own, ((pool_reach, pool_reach), (0, 0)))
        pooled = pool_group(extended, own, positions, 2 ** group, seq_total)
        pool_parts.append(jnp.dot(pooled, pool_mix_weight[group], preferred_element_type=jnp.float32).astype(jnp.bfloat16))
    pool_out = jnp.concatenate(pool_parts, 1)
    grp = HQ // KVH
    query_heads = rot_query.reshape(seq_total, KVH, grp, HD)
    key_pad = jnp.pad(rot_key.reshape(seq_total, KVH, HD), ((WINDOW, WINDOW), (0, 0), (0, 0)))
    value_pad = jnp.pad(value.reshape(seq_total, KVH, HD), ((WINDOW, WINDOW), (0, 0), (0, 0)))
    sink = sink_logit.reshape(KVH, grp)
    block_rows = 512

    def block_fn(block_index):
        start = (block_index * block_rows).astype(jnp.int32)
        queries = lax.dynamic_slice_in_dim(query_heads, start, block_rows, 0)
        keys = lax.dynamic_slice_in_dim(key_pad, start, block_rows + 2 * WINDOW, 0)
        values = lax.dynamic_slice_in_dim(value_pad, start, block_rows + 2 * WINDOW, 0)
        query_pos = start + jnp.arange(block_rows, dtype=jnp.int32)
        key_pos = start - WINDOW + jnp.arange(block_rows + 2 * WINDOW, dtype=jnp.int32)
        return attend_block(queries, keys, values, sink, query_pos, key_pos, seq_total)
    n_blocks = seq_total // block_rows
    attended, log_blocks = lax.map(block_fn, jnp.arange(n_blocks, dtype=jnp.int32))
    attended = attended.reshape(seq_total, HQ * HD)
    log_weight = jnp.moveaxis(log_blocks.reshape(n_blocks, HQ, block_rows), 0, 1).reshape(HQ, seq_total)
    attn_group = HQ * HD // N_TP
    mixed = jnp.zeros((seq_total, D), jnp.float32)
    for part in range(N_TP):
        term = jnp.dot(pool_out[:, part * POOL_GC:(part + 1) * POOL_GC], out_pool_weight[part * POOL_GC:(part + 1) * POOL_GC], preferred_element_type=jnp.float32)
        term = term + jnp.dot(attended[:, part * attn_group:(part + 1) * attn_group], out_attn_weight[part * attn_group:(part + 1) * attn_group], preferred_element_type=jnp.float32)
        rounded = lax.optimization_barrier(term.astype(jnp.bfloat16))
        mixed = mixed + rounded.astype(jnp.float32)
    return (mixed.astype(jnp.bfloat16), log_weight)
```

```python
import jax
import jax.numpy as jnp
from jax import lax
from jax.sharding import Mesh
from jax.experimental import pallas as pl
from jax.experimental.pallas import tpu as pltpu
from jax.sharding import PartitionSpec as P

HD = 64
WINDOW = 128
GRID_W = 64
SP = ("sp_0", "sp_1", "sp_2")


norm_eps = 1e-06
rope_base = 10000.0
pool_reach = 8
neg_fill = -1e30


def with_halo(cells, sides, width):
    for axis, dim in sides:
        count = lax.axis_size(axis)
        ends = count - 1
        head = lax.slice_in_dim(cells, 0, width, axis=dim)
        tail = lax.slice_in_dim(cells, cells.shape[dim] - width, cells.shape[dim], axis=dim)
        cells = jnp.concatenate(
            [
                lax.ppermute(tail, axis, [(i, (i + 1) % count) for i in range(ends)]),
                cells,
                lax.ppermute(head, axis, [((i + 1) % count, i) for i in range(ends)]),
            ],
            axis=dim,
        )
    return cells


def in_blocks(shard, dim, count):
    lengths = shard.shape
    blocks = shard.reshape(*lengths[:dim], count, lengths[dim] // count, *lengths[dim + 1 :])
    return jnp.moveaxis(blocks, dim, 0)


def summed_on_arrival(shard, axis, dim):
    count = lax.axis_size(axis)
    blocks = lax.all_to_all(in_blocks(shard, dim, count), axis, 0, 0, tiled=True)
    return jnp.sum(blocks.astype(jnp.float32), axis=0)


MESH = pl.DeviceIdType.MESH
AX_Z, AX_Y, AX_C, AX_X = "sp_0", "sp_1", "sp_2", "tp"


def remote(src, dst, send_sem, recv_sem, device):
    return pltpu.make_async_remote_copy(
        src_ref=src,
        dst_ref=dst,
        send_sem=send_sem,
        recv_sem=recv_sem,
        device_id=device,
        device_id_type=MESH,
    )


def wait_bytes(ref, sem):
    pltpu.make_async_copy(ref, ref, sem).wait()


class Torus:
    def __init__(self, buf, first, sems):
        self.buf, self.first = buf, first
        self.p1_send, self.p1_recv, self.p2_send, self.p2_recv, self.d_send, self.d_recv = sems
        self.z, self.y, self.c = lax.axis_index(AX_Z), lax.axis_index(AX_Y), lax.axis_index(AX_C)
        self.n1 = buf.shape[1] if first == AX_Y else buf.shape[0]
        self.n2 = buf.shape[0] if first == AX_Y else buf.shape[1]
        self.a = self.y if first == AX_Y else self.z
        self.b = self.z if first == AX_Y else self.y
        self.second = AX_Z if first == AX_Y else AX_Y

    def own(self):
        return self.buf.at[self.z, self.y, self.c]

    def chunk(self, b, start, size):
        if self.first == AX_Y:
            return self.buf.at[b, start : start + size, self.c]
        return self.buf.at[start : start + size, b, self.c]

    def hops(self, way, group):
        half = self.n2 // 2
        return half if (way == 0) == (group == 0) else half - 1

    def phase1_start(self):
        for d in range(1, self.n1):
            remote(
                self.own(), self.own(), self.p1_send, self.p1_recv,
                {self.first: lax.rem(self.a + d, self.n1)},
            ).start()

    def phase1_wait(self):
        wait_bytes(self.chunk(self.b, 0, self.n1 - 1), self.p1_recv)
        self.to_partner(self.chunk(self.b, 0, self.n1))

    def to_partner(self, ref):
        remote(ref, ref, self.d_send, self.d_recv, {AX_C: 1 - self.c}).start()

    def relay(self, way, group, hop):
        step = 1 if way == 0 else self.n2 - 1
        origin = lax.rem(self.b + (hop - 1) * (self.n2 - step), self.n2)
        size = self.n1 // 2
        ref = self.chunk(origin, group * size, size)
        return remote(
            ref, ref, self.p2_send.at[way, group, hop - 1], self.p2_recv.at[way, group, hop - 1],
            {self.second: lax.rem(self.b + step, self.n2)},
        )

    def arrived(self, way, group, hop):
        step = 1 if way == 0 else self.n2 - 1
        origin = lax.rem(self.b + hop * (self.n2 - step), self.n2)
        size = self.n1 // 2
        ref = self.chunk(origin, group * size, size)
        wait_bytes(ref, self.p2_recv.at[way, group, hop - 1])
        self.to_partner(ref)

    def level(self, hop):
        for group in range(2):
            for way in range(2):
                last = self.hops(way, group)
                if 1 < hop <= last + 1:
                    self.arrived(way, group, hop - 1)
                if hop <= last:
                    self.relay(way, group, hop).start()

    def levels(self):
        return self.n2 // 2 + 1

    def finish(self):
        wait_bytes(self.buf.at[:, :, 1 - self.c], self.d_recv)
        wait_bytes(self.buf.at[:, :, self.c], self.d_send)
        wait_bytes(self.chunk(self.b, 0, self.n1 - 1), self.p1_send)
        for group in range(2):
            for way in range(2):
                for hop in range(1, self.hops(way, group) + 1):
                    self.relay(way, group, hop).wait_send()


def torus_sems(n2):
    dma = pltpu.SemaphoreType.DMA
    hops = max(n2 // 2, 1)
    return [dma(()), dma(()), dma((2, 2, hops)), dma((2, 2, hops)), dma(()), dma(())]


class Ring:
    def __init__(self, buf, sems):
        self.buf = buf
        self.send, self.recv = sems
        self.n, self.x = buf.shape[0], lax.axis_index(AX_X)
        self.half = buf.shape[1] // 2

    def part(self, x, which):
        return self.buf.at[x, which * self.half : (which + 1) * self.half]

    def copy(self, way, index, x, which):
        step = 1 if way == 0 else self.n - 1
        ref = self.part(x, which)
        return remote(
            ref, ref, self.send.at[way, index], self.recv.at[way, index],
            {AX_X: lax.rem(self.x + step, self.n)},
        )

    def start(self):
        for index in range(2):
            for way in range(2):
                self.copy(way, index, self.x, index if way == 0 else 1 - index).start()

    def forward(self):
        for way in range(2):
            step = 1 if way == 0 else self.n - 1
            behind = lax.rem(self.x + self.n - step, self.n)
            which = way
            wait_bytes(self.part(behind, which), self.recv.at[way, 0])
            self.copy(way, 2, behind, which).start()

    def finish(self):
        for way in range(2):
            step = 1 if way == 0 else self.n - 1
            behind = lax.rem(self.x + self.n - step, self.n)
            across = lax.rem(self.x + 2, self.n)
            wait_bytes(self.part(behind, 1 - way), self.recv.at[way, 1])
            wait_bytes(self.part(across, way), self.recv.at[way, 2])
        for way in range(2):
            for index in range(3):
                self.copy(way, index, self.x, 0).wait_send()


def greet(peers):
    barrier = pltpu.get_barrier_semaphore()
    for peer in peers:
        pl.semaphore_signal(barrier, inc=1, device_id=peer, device_id_type=MESH)
    pl.semaphore_wait(barrier, len(peers))


def all_peers(nz, ny, nx):
    z, y, c, x = (lax.axis_index(a) for a in (AX_Z, AX_Y, AX_C, AX_X))
    peers = [{AX_C: 1 - c}]
    peers += [{AX_X: lax.rem(x + d, nx)} for d in (1, nx - 1)]
    peers += [{AX_Y: lax.rem(y + d, ny)} for d in range(1, ny)]
    peers += [{AX_Z: lax.rem(z + d, nz)} for d in range(1, nz)]
    return peers


def gather_kernel(
    tok_ref, q_ref, k_ref, v_ref, p_ref, oa_ref, ob_ref,
    t_buf, wa, wb, oa, ob, load_sem, ring_send, ring_recv, *torus,
):
    z, y, c, x = (lax.axis_index(a) for a in (AX_Z, AX_Y, AX_C, AX_X))
    ring = Ring(t_buf, (ring_send, ring_recv))
    in_a = Torus(wa, AX_Y, torus[0:6])
    in_b = Torus(wb, AX_Z, torus[6:12])
    out_a = Torus(oa, AX_Y, torus[12:18])
    out_b = Torus(ob, AX_Z, torus[18:24])
    loads = [
        pltpu.make_async_copy(tok_ref, t_buf.at[x], load_sem.at[0]),
        pltpu.make_async_copy(q_ref, wa.at[z, y, c], load_sem.at[1]),
        pltpu.make_async_copy(k_ref, wb.at[z, y, c, :, 0:128], load_sem.at[2]),
        pltpu.make_async_copy(v_ref, wb.at[z, y, c, :, 128:256], load_sem.at[3]),
        pltpu.make_async_copy(p_ref, wb.at[z, y, c, :, 256:512], load_sem.at[4]),
        pltpu.make_async_copy(oa_ref, oa.at[z, y, c], load_sem.at[5]),
        pltpu.make_async_copy(ob_ref, ob.at[z, y, c], load_sem.at[6]),
    ]
    for load in loads:
        load.start()
    greet(all_peers(wa.shape[0], wa.shape[1], t_buf.shape[0]))
    for load in loads:
        load.wait()
    ring.start()
    in_a.phase1_start()
    in_b.phase1_start()
    in_a.phase1_wait()
    in_b.phase1_wait()
    for hop in range(1, in_a.levels() + 1):
        in_a.level(hop)
        in_b.level(hop)
        if hop == 2:
            ring.forward()
        if hop == in_a.levels() - 1:
            out_a.phase1_start()
            out_b.phase1_start()
    out_a.phase1_wait()
    out_b.phase1_wait()
    for hop in range(1, out_a.levels() + 1):
        out_a.level(hop)
        out_b.level(hop)
    ring.finish()
    in_a.finish()
    in_b.finish()
    out_a.finish()
    out_b.finish()


def gather_all(tokens, weights, out_a, out_b):
    nz, ny, nc, nx = (lax.axis_size(a) for a in (AX_Z, AX_Y, AX_C, AX_X))
    rows, width = tokens.shape
    bf = jnp.bfloat16
    shapes = [
        jax.ShapeDtypeStruct((nx, rows, width), bf),
        jax.ShapeDtypeStruct((nz, ny, nc, 16, 512), bf),
        jax.ShapeDtypeStruct((nz, ny, nc, 16, 512), bf),
        jax.ShapeDtypeStruct((nz, ny, nc, 16, 384), bf),
        jax.ShapeDtypeStruct((nz, ny, nc, 16, 384), bf),
    ]
    dma = pltpu.SemaphoreType.DMA
    return pl.pallas_call(
        gather_kernel,
        out_shape=shapes,
        in_specs=[pl.BlockSpec(memory_space=pl.ANY)] * 7,
        out_specs=[pl.BlockSpec(memory_space=pltpu.VMEM)] * 5,
        scratch_shapes=[dma((7,)), dma((2, 3)), dma((2, 3))]
        + torus_sems(nz) + torus_sems(ny) + torus_sems(nz) + torus_sems(ny),
        compiler_params=pltpu.CompilerParams(
            collective_id=0, has_side_effects=True, vmem_limit_bytes=40 * 1024 * 1024
        ),
    )(tokens, *weights, out_a, out_b)


def rope_tables(positions, head_dim):
    n_freq = head_dim // 4
    freqs = rope_base ** (-jnp.arange(n_freq, dtype=jnp.float32) / n_freq)
    rows = (positions // GRID_W).astype(jnp.float32)
    columns = (positions % GRID_W).astype(jnp.float32)
    row_angle = rows[:, None] * freqs[None, :]
    col_angle = columns[:, None] * freqs[None, :]
    return (jnp.cos(row_angle), jnp.sin(row_angle), jnp.cos(col_angle), jnp.sin(col_angle))


def rotate_half(values, cosine, sine):
    middle = values.shape[-1] // 2
    first = values[..., :middle]
    second = values[..., middle:]
    return jnp.concatenate([first * cosine - second * sine, second * cosine + first * sine], -1)


def rotate_heads(values, tables, head_dim):
    rows_count = values.shape[0]
    shaped = values.astype(jnp.float32).reshape(rows_count, -1, head_dim)
    cos_r, sin_r, cos_c, sin_c = [table[:, None, :] for table in tables]
    split = head_dim // 2
    turned = jnp.concatenate(
        [
            rotate_half(shaped[..., :split], cos_r, sin_r),
            rotate_half(shaped[..., split:], cos_c, sin_c),
        ],
        -1,
    )
    return turned.reshape(rows_count, -1).astype(jnp.bfloat16)


def pool_group(extended, own, positions, half_width, seq_total):
    rows_count = own.shape[0]
    summed = jnp.zeros(own.shape, jnp.float32)
    counted = jnp.zeros((rows_count,), jnp.float32)
    for shift_by in range(-pool_reach, pool_reach):
        source = positions + shift_by
        inside = (
            (shift_by >= -half_width)
            & (shift_by < half_width)
            & (source >= 0)
            & (source < seq_total)
        )
        window_rows = extended[pool_reach + shift_by : pool_reach + shift_by + rows_count].astype(
            jnp.float32
        )
        summed = summed + jnp.where(inside[:, None], window_rows, 0.0)
        counted = counted + inside.astype(jnp.float32)
    return (summed / counted[:, None] - own.astype(jnp.float32)).astype(jnp.bfloat16)


def attend_block(queries, keys, values, sink, query_pos, key_pos, seq_total):
    scores = jnp.einsum(
        "qhgd,khd->hgqk", queries, keys, preferred_element_type=jnp.float32
    ) * HD ** (-0.5)
    valid = (
        (jnp.abs(query_pos[:, None] - key_pos[None, :]) <= WINDOW)
        & (key_pos >= 0)[None, :]
        & (key_pos < seq_total)[None, :]
    )
    scores = jnp.where(valid, scores, neg_fill)
    row_top = jnp.maximum(jnp.max(scores, -1), sink[:, :, None])
    exps = jnp.exp(scores - row_top[..., None])
    row_total = jnp.sum(exps, -1) + jnp.exp(sink[:, :, None] - row_top)
    weights = (exps / row_total[..., None]).astype(jnp.bfloat16)
    attended = jnp.einsum("hgqk,khd->qhgd", weights, values, preferred_element_type=jnp.float32)
    return (attended.astype(jnp.bfloat16), row_top + jnp.log(row_total))


def local(
    tokens,
    norm_gain,
    query_weight,
    key_weight,
    value_weight,
    pool_in_weight,
    pool_mix_weight,
    sink_logit,
    out_pool_weight,
    out_attn_weight,
):
    out_rows = jnp.concatenate([out_pool_weight, out_attn_weight], 0).T
    blocks, wa, wb, oa, ob = gather_all(
        tokens,
        (query_weight, key_weight, value_weight, pool_in_weight),
        out_rows[:, :384],
        out_rows[:, 384:],
    )
    whole = jnp.moveaxis(blocks, 0, 1).reshape(blocks.shape[1], -1)
    wide = whole.astype(jnp.float32)
    normed = (
        wide * lax.rsqrt(jnp.mean(wide * wide, -1, keepdims=True) + norm_eps) * norm_gain
    ).astype(jnp.bfloat16)
    tok_rows = normed.shape[0]
    seq_total = tok_rows * lax.axis_size(SP)
    offset = lax.axis_index(SP) * tok_rows
    weight_a, weight_b = wa.reshape(-1, 512), wb.reshape(-1, 512)
    pieces = (weight_a, weight_b[:, :128], weight_b[:, 128:256], weight_b[:, 256:])
    sums = tuple((jnp.dot(normed, piece, preferred_element_type=jnp.float32) for piece in pieces))
    query, key, value, pool_input = [total.astype(jnp.bfloat16) for total in sums]
    positions = offset + jnp.arange(tok_rows, dtype=jnp.int32)
    tables = rope_tables(positions, HD)
    rot_query = rotate_heads(query, tables, HD)
    rot_key = rotate_heads(key, tables, HD)
    chans = pool_input.shape[1]
    key_width = rot_key.shape[1]
    joined = jnp.concatenate([pool_input, rot_key, value], 1)
    extended = with_halo(joined, ((SP, 0),), WINDOW)
    pool_ext = extended[WINDOW - pool_reach : WINDOW + tok_rows + pool_reach, :chans]
    key_ext = extended[:, chans : chans + key_width]
    value_ext = extended[:, chans + key_width :]
    half_width = jnp.left_shift(jnp.int32(1), lax.axis_index("tp"))
    pooled = pool_group(pool_ext, pool_input, positions, half_width, seq_total)
    pool_out = jnp.dot(pooled, pool_mix_weight[0], preferred_element_type=jnp.float32).astype(
        jnp.bfloat16
    )
    heads_local = rot_query.shape[1] // HD
    kv_local = key_width // HD
    grp = heads_local // kv_local
    query_heads = rot_query.reshape(tok_rows, kv_local, grp, HD)
    key_heads = key_ext.reshape(-1, kv_local, HD)
    value_heads = value_ext.reshape(-1, kv_local, HD)
    sink = sink_logit.reshape(kv_local, grp)
    block_rows = min(tok_rows, 256)
    attended_parts = []
    log_parts = []
    for block_index in range(tok_rows // block_rows):
        start = block_index * block_rows
        query_pos = offset + start + jnp.arange(block_rows, dtype=jnp.int32)
        key_pos = offset + start - WINDOW + jnp.arange(block_rows + 2 * WINDOW, dtype=jnp.int32)
        attended_block, log_block = attend_block(
            query_heads[start : start + block_rows],
            key_heads[start : start + block_rows + 2 * WINDOW],
            value_heads[start : start + block_rows + 2 * WINDOW],
            sink,
            query_pos,
            key_pos,
            seq_total,
        )
        attended_parts.append(attended_block.reshape(block_rows, heads_local * HD))
        log_parts.append(log_block.reshape(heads_local, block_rows))
    attended = jnp.concatenate(attended_parts, 0)
    log_weight = jnp.concatenate(log_parts, 1)
    features = jnp.concatenate([pool_out, attended], 1)
    outs = (((1,), (1,)), ((), ()))
    term = lax.dot_general(
        features[:, :384], oa.reshape(-1, 384), outs, preferred_element_type=jnp.float32
    ) + lax.dot_general(
        features[:, 384:], ob.reshape(-1, 384), outs, preferred_element_type=jnp.float32
    )
    mixed = summed_on_arrival(term.astype(jnp.bfloat16), "tp", 1).astype(jnp.bfloat16)
    return (mixed, log_weight)


def solution(mesh):
    finer = Mesh(mesh.devices.reshape(8, 8, 2, mesh.shape["tp"]), ("sp_0", "sp_1", "sp_2", "tp"))
    placed = (
        P(SP, "tp"),
        P(),
        P(SP, "tp"),
        P(SP, "tp"),
        P(SP, "tp"),
        P(SP, "tp"),
        P("tp", None, None),
        P("tp"),
        P("tp", SP),
        P("tp", SP),
    )
    return jax.shard_map(
        local, mesh=finer, in_specs=placed, out_specs=(P(SP, "tp"), P("tp", SP)), check_vma=False
    )
```

```python
import jax
import jax.numpy as jnp
from jax import lax
from jax.sharding import Mesh
from jax.experimental import pallas as pl
from jax.experimental.pallas import tpu as pltpu
from jax.sharding import PartitionSpec as P

HD = 64
GRID_W = 64
SP = ("sp_0", "sp_1", "sp_2")


norm_eps = 1e-06
rope_base = 10000.0
neg_fill = -1e30


def rope_tables(positions, head_dim):
    n_freq = head_dim // 4
    freqs = rope_base ** (-jnp.arange(n_freq, dtype=jnp.float32) / n_freq)
    rows = (positions // GRID_W).astype(jnp.float32)
    columns = (positions % GRID_W).astype(jnp.float32)
    row_angle = rows[:, None] * freqs[None, :]
    col_angle = columns[:, None] * freqs[None, :]
    return (jnp.cos(row_angle), jnp.sin(row_angle), jnp.cos(col_angle), jnp.sin(col_angle))


MESH = pl.DeviceIdType.MESH
AX_Z, AX_Y, AX_C, AX_X = "sp_0", "sp_1", "sp_2", "tp"
BLOCK = 128
EDGE = 16


def remote(src, dst, send_sem, recv_sem, device):
    return pltpu.make_async_remote_copy(
        src_ref=src,
        dst_ref=dst,
        send_sem=send_sem,
        recv_sem=recv_sem,
        device_id=device,
        device_id_type=MESH,
    )


def wait_bytes(ref, sem):
    pltpu.make_async_copy(ref, ref, sem).wait()


class Torus:
    def __init__(self, buf, first, size, sems):
        self.buf, self.first, self.size = buf, first, size
        self.p1_send, self.p1_recv, self.p2_send, self.p2_recv, self.d_send, self.d_recv = sems
        self.z, self.y, self.c = lax.axis_index(AX_Z), lax.axis_index(AX_Y), lax.axis_index(AX_C)
        by_y = first == AX_Y
        self.n1, self.n2 = (buf.shape[1], buf.shape[0]) if by_y else (buf.shape[0], buf.shape[1])
        self.a, self.b = (self.y, self.z) if by_y else (self.z, self.y)
        self.second = AX_Z if by_y else AX_Y
        self.groups = self.n1 // size

    def chunk(self, b, start, size):
        if self.first == AX_Y:
            return self.buf.at[b, pl.ds(start, size), self.c]
        return self.buf.at[pl.ds(start, size), b, self.c]

    def group_id(self, k):
        return lax.rem(lax.div(self.a, self.size) + k, self.groups)

    def hops(self, way, k):
        half = self.n2 // 2
        return half if (way == 0) == (k < self.groups // 2) else half - 1

    def phase1_start(self):
        own = self.buf.at[self.z, self.y, self.c]
        order = sorted(range(1, self.n1), key=lambda d: min(d, self.n1 - d))
        for d in order:
            remote(
                own, own, self.p1_send, self.p1_recv.at[self.group_id(0)],
                {self.first: lax.rem(self.a + d, self.n1)},
            ).start()

    def to_partner(self, ref):
        remote(ref, ref, self.d_send, self.d_recv, {AX_C: 1 - self.c}).start()

    def phase1_group(self, k):
        count = self.size - 1 if k == 0 else self.size
        wait_bytes(self.chunk(self.b, 0, count), self.p1_recv.at[self.group_id(k)])
        for way in range(2):
            self.relay(way, k, 1).start()
        self.to_partner(self.chunk(self.b, self.group_id(k) * self.size, self.size))

    def block(self, way, k, back):
        step = 1 if way == 0 else self.n2 - 1
        origin = lax.rem(self.b + back * (self.n2 - step), self.n2)
        return self.chunk(origin, self.group_id(k) * self.size, self.size)

    def relay(self, way, k, hop):
        step = 1 if way == 0 else self.n2 - 1
        ref = self.block(way, k, hop - 1)
        return remote(
            ref, ref, self.p2_send.at[way, k, hop - 1], self.p2_recv.at[way, k, hop - 1],
            {self.second: lax.rem(self.b + step, self.n2)},
        )

    def level(self, hop, k, way):
        last = self.hops(way, k)
        if hop > last + 1:
            return
        ref = self.block(way, k, hop - 1)
        wait_bytes(ref, self.p2_recv.at[way, k, hop - 2])
        if hop <= last:
            self.relay(way, k, hop).start()
        self.to_partner(ref)

    def arrived(self):
        wait_bytes(self.buf.at[:, :, 1 - self.c], self.d_recv)

    def drain(self):
        wait_bytes(self.buf.at[:, :, self.c], self.d_send)
        wait_bytes(self.chunk(self.b, 0, self.n1 - 1), self.p1_send)
        for k in range(self.groups):
            for way in range(2):
                for hop in range(1, self.hops(way, k) + 1):
                    self.relay(way, k, hop).wait_send()


def torus_sems(n1, n2, size):
    dma = pltpu.SemaphoreType.DMA
    groups, hops = n1 // size, n2 // 2
    return [
        dma(()), dma((groups,)), dma((2, groups, hops)), dma((2, groups, hops)), dma(()), dma(()),
    ]


class Ring:
    def __init__(self, buf, sems):
        self.buf = buf
        self.send, self.recv = sems
        self.n, self.x = buf.shape[0], lax.axis_index(AX_X)
        self.half = buf.shape[1] // 2

    def part(self, x, which):
        return self.buf.at[x, which * self.half : (which + 1) * self.half]

    def copy(self, way, index, x, which):
        step = 1 if way == 0 else self.n - 1
        ref = self.part(x, which)
        return remote(
            ref, ref, self.send.at[way, index], self.recv.at[way, index],
            {AX_X: lax.rem(self.x + step, self.n)},
        )

    def start(self):
        for index in range(2):
            for way in range(2):
                self.copy(way, index, self.x, index if way == 0 else 1 - index).start()

    def forward(self):
        for way in range(2):
            step = 1 if way == 0 else self.n - 1
            behind = lax.rem(self.x + self.n - step, self.n)
            wait_bytes(self.part(behind, way), self.recv.at[way, 0])
            self.copy(way, 2, behind, way).start()

    def arrived(self):
        for way in range(2):
            step = 1 if way == 0 else self.n - 1
            behind = lax.rem(self.x + self.n - step, self.n)
            across = lax.rem(self.x + 2, self.n)
            wait_bytes(self.part(behind, 1 - way), self.recv.at[way, 1])
            wait_bytes(self.part(across, way), self.recv.at[way, 2])

    def drain(self):
        for way in range(2):
            for index in range(3):
                self.copy(way, index, self.x, 0).wait_send()


def sequence_neighbour(step):
    nz, ny, nc = (lax.axis_size(a) for a in (AX_Z, AX_Y, AX_C))
    place = (lax.axis_index(AX_Z) * ny + lax.axis_index(AX_Y)) * nc + lax.axis_index(AX_C)
    place = lax.rem(place + step + nz * ny * nc, nz * ny * nc)
    chip = lax.div(place, nc)
    return {AX_Z: lax.div(chip, ny), AX_Y: lax.rem(chip, ny), AX_C: lax.rem(place, nc)}


def greet_all():
    nz, ny, nx = (lax.axis_size(a) for a in (AX_Z, AX_Y, AX_X))
    z, y, c, x = (lax.axis_index(a) for a in (AX_Z, AX_Y, AX_C, AX_X))
    peers = [sequence_neighbour(1), sequence_neighbour(-1), {AX_C: 1 - c}]
    peers += [{AX_X: lax.rem(x + d, nx)} for d in (1, nx - 1)]
    peers += [{AX_Y: lax.rem(y + d, ny)} for d in range(1, ny)]
    peers += [{AX_Z: lax.rem(z + d, nz)} for d in range(1, nz)]
    barrier = pltpu.get_barrier_semaphore()
    for peer in peers:
        pl.semaphore_signal(barrier, inc=1, device_id=peer, device_id_type=MESH)
    pl.semaphore_wait(barrier, len(peers))


def turned(values, cosine, sine):
    lane = lax.broadcasted_iota(jnp.int32, values.shape, 1)
    ahead = pltpu.roll(values, 112, 1)
    behind = pltpu.roll(values, 16, 1)
    return values * cosine + jnp.where(lax.rem(lane, 32) < 16, ahead, behind) * sine


def rounded(values):
    return values.astype(jnp.bfloat16).astype(jnp.float32)


def rows_of(buf, start, size, columns):
    parts = buf[start // 256 : (start + size) // 256, :, :, :, columns]
    return parts.reshape(size, -1)


def normalise(t_buf, gain_ref, normed):
    def step(i, carry):
        rows = pl.ds(pl.multiple_of(i * BLOCK, BLOCK), BLOCK)
        parts = [t_buf[k, rows, :].astype(jnp.float32) for k in range(4)]
        total = sum(jnp.sum(p * p, axis=-1, keepdims=True) for p in parts)
        scale = lax.rsqrt(total / 2048.0 + norm_eps)
        for k in range(4):
            cols = slice(k * 512, (k + 1) * 512)
            normed[rows, cols] = (parts[k] * scale * gain_ref[0:1, cols]).astype(jnp.bfloat16)
        return carry

    lax.fori_loop(0, 4, step, 0)


def project_keys(normed, wb, cos_ref, sin_ref, kv_ext):
    both = jnp.dot(
        normed[...], rows_of(wb, 0, 2048, slice(0, 256)), preferred_element_type=jnp.float32
    )
    keys = turned(rounded(both[:, :128]), cos_ref[...], sin_ref[...])
    kv_ext[BLOCK : BLOCK + 512, 0:128] = keys.astype(jnp.bfloat16)
    kv_ext[BLOCK : BLOCK + 512, 128:256] = both[:, 128:].astype(jnp.bfloat16)


def project_pool(normed, wb, pool_ext):
    pool_ext[EDGE : EDGE + 512, :] = jnp.dot(
        normed[...], rows_of(wb, 0, 2048, slice(256, 512)), preferred_element_type=jnp.float32
    ).astype(jnp.bfloat16)


def project_queries(normed, wa, cos_ref, sin_ref, queries, h):
    cols = slice(h * 256, (h + 1) * 256)
    found = jnp.dot(normed[...], rows_of(wa, 0, 2048, cols), preferred_element_type=jnp.float32)
    for pair in range(2):
        values = turned(
            rounded(found[:, pair * 128 : (pair + 1) * 128]), cos_ref[...], sin_ref[...]
        ) * (HD**-0.5)
        lane = lax.broadcasted_iota(jnp.int32, values.shape, 1)
        mine = (lane < 64) if h == 0 else (lane >= 64)
        for odd in range(2):
            placed = values if odd == h else pltpu.roll(values, 64, 1)
            placed = jnp.where(mine, placed, 0.0).astype(jnp.bfloat16)
            g = pair * 2 + odd
            for b in range(4):
                queries[h, b, g * BLOCK : (g + 1) * BLOCK, :] = placed[b * BLOCK : (b + 1) * BLOCK]


def attend(b, h, place, places, kv_ext, queries, sink_ref, features, log_ref):
    start = pl.multiple_of(b * BLOCK, BLOCK)
    keys = kv_ext[pl.ds(start, 3 * BLOCK), 0:128]
    scores = lax.dot_general(
        keys, queries[h, b], (((1,), (1,)), ((), ())), preferred_element_type=jnp.float32
    )
    shape = (BLOCK, 4 * BLOCK)
    key = lax.broadcasted_iota(jnp.int32, shape, 0)
    query = lax.rem(lax.broadcasted_iota(jnp.int32, shape, 1), BLOCK)
    first = jnp.where((place == 0) & (b == 0), BLOCK, 0)
    last = jnp.where((place == places - 1) & (b == 3), -1, BLOCK)
    before = jnp.where(key >= jnp.maximum(query, first), scores[:BLOCK], neg_fill)
    here = scores[BLOCK : 2 * BLOCK]
    after = jnp.where(key <= jnp.minimum(query, last), scores[2 * BLOCK :], neg_fill)
    sink = sink_ref[h : h + 1, :]
    top = jnp.max(jnp.maximum(jnp.maximum(before, here), after), axis=0, keepdims=True)
    top = jnp.maximum(top, sink)
    exps = [jnp.exp(part - top) for part in (before, here, after)]
    total = jnp.sum(exps[0] + exps[1] + exps[2], axis=0, keepdims=True) + jnp.exp(sink - top)
    logs = top + jnp.log(total)
    weights = jnp.concatenate([e.astype(jnp.bfloat16) for e in exps], axis=0)
    values = kv_ext[pl.ds(start, 3 * BLOCK), 128:256]
    summed = lax.dot_general(
        values, weights, (((0,), (0,)), ((), ())), preferred_element_type=jnp.float32
    )
    mine = summed[h * 64 : (h + 1) * 64] / total
    for g in range(4):
        log_ref[4 * h + g : 4 * h + g + 1, pl.ds(start, BLOCK)] = logs[
            :, g * BLOCK : (g + 1) * BLOCK
        ]
    for pair in range(2):
        two = jnp.concatenate(
            [mine[:, (2 * pair + e) * BLOCK : (2 * pair + e + 1) * BLOCK] for e in range(2)], axis=0
        )
        at = 256 + h * 256 + pair * 128
        features[pl.ds(start, BLOCK), at : at + 128] = two.T.astype(jnp.bfloat16)


def pool(b, place, places, reach, pool_ext, mix_ref, features):
    start = pl.multiple_of(b * BLOCK, BLOCK)
    size = BLOCK + 2 * EDGE
    base = place * 512 + b * BLOCK
    row = lax.broadcasted_iota(jnp.int32, (BLOCK, size), 0)
    col = lax.broadcasted_iota(jnp.int32, (BLOCK, size), 1) - EDGE
    inside = (col >= row - reach) & (col < row + reach)
    inside = inside & (col >= -base) & (col < places * 512 - base)
    band = jnp.where(inside, 1.0, 0.0)
    counted = jnp.sum(band, axis=-1, keepdims=True)
    ext = pool_ext[pl.ds(start, size), :]
    summed = jnp.dot(band.astype(jnp.bfloat16), ext, preferred_element_type=jnp.float32)
    own = ext[EDGE : EDGE + BLOCK].astype(jnp.float32)
    pooled = (summed / counted - own).astype(jnp.bfloat16)
    features[pl.ds(start, BLOCK), 0:256] = jnp.dot(
        pooled, mix_ref[0], preferred_element_type=jnp.float32
    ).astype(jnp.bfloat16)


def partial_term(b, j, features, oa, ob):
    rows = pl.ds(pl.multiple_of(b * BLOCK, BLOCK), BLOCK)
    dims = (((1,), (1,)), ((), ()))
    low = oa[pl.ds(2 * j, 2)].reshape(512, 384)
    high = ob[pl.ds(2 * j, 2)].reshape(512, 384)
    return lax.dot_general(
        features[rows, 0:384], low, dims, preferred_element_type=jnp.float32
    ) + lax.dot_general(features[rows, 384:768], high, dims, preferred_element_type=jnp.float32)


class Scatter:
    def __init__(self, refs, sems):
        self.far, self.near, self.far_in, self.near_in, self.kept = refs
        self.far_send, self.far_recv, self.near_send, self.near_recv = sems
        self.n, self.x = lax.axis_size(AX_X), lax.axis_index(AX_X)
        self.half = BLOCK // 2

    def target(self, way):
        return lax.rem(self.x + (1 if way == 0 else self.n - 1), self.n)

    def far_copy(self, b, way):
        rows = slice(way * self.half, (way + 1) * self.half)
        return remote(
            self.far.at[b, rows], self.far_in.at[b, way],
            self.far_send.at[b, way], self.far_recv.at[b, way], {AX_X: self.target(way)},
        )

    def near_copy(self, b, way, added):
        which = way if added else 1 - way
        rows = slice(which * self.half, (which + 1) * self.half)
        index = 1 if added else 0
        return remote(
            self.near.at[b, way, rows], self.near_in.at[b, way, rows],
            self.near_send.at[b, way, index], self.near_recv.at[b, way, index],
            {AX_X: self.target(way)},
        )

    def compute(self, b, features, oa, ob):
        across = lax.rem(self.x + 2, self.n)
        self.far[b] = partial_term(b, across, features, oa, ob).astype(jnp.bfloat16)
        for way in range(2):
            self.near[b, way] = partial_term(b, self.target(way), features, oa, ob).astype(jnp.bfloat16)
            self.far_copy(b, way).start()
        self.kept[b] = partial_term(b, self.x, features, oa, ob).astype(jnp.bfloat16)
        for way in range(2):
            self.near_copy(b, way, False).start()

    def add(self, b):
        for way in range(2):
            rows = slice(way * self.half, (way + 1) * self.half)
            self.far_copy(b, way).wait_recv()
            both = self.near[b, way, rows].astype(jnp.float32) + self.far_in[b, way].astype(jnp.float32)
            self.near[b, way, rows] = both.astype(jnp.bfloat16)
        for way in range(2):
            self.near_copy(b, way, True).start()

    def finish(self, b, out_ref):
        for way in range(2):
            for added in (False, True):
                self.near_copy(b, way, added).wait_recv()
        total = self.kept[b].astype(jnp.float32)
        for way in range(2):
            total = total + self.near_in[b, way].astype(jnp.float32)
        out_ref[pl.ds(pl.multiple_of(b * BLOCK, BLOCK), BLOCK), :] = total.astype(jnp.bfloat16)

    def drain(self, b):
        for way in range(2):
            self.far_copy(b, way).wait_send()
            for added in (False, True):
                self.near_copy(b, way, added).wait_send()


def layer_kernel(
    tok_ref, q_ref, k_ref, v_ref, p_ref, oa_ref, ob_ref,
    gain_ref, mix_ref, sink_ref, cos_ref, sin_ref,
    out_ref, log_ref,
    t_buf, wa, wb, oa, ob, normed, queries, kv_ext, pool_ext, features,
    far, near, far_in, near_in, kept,
    load_sem, ring_send, ring_recv, halo_send, halo_recv, far_send, far_recv, near_send, near_recv,
    *torus,
):
    z, y, c, x = (lax.axis_index(a) for a in (AX_Z, AX_Y, AX_C, AX_X))
    nz, ny, nc = (lax.axis_size(a) for a in (AX_Z, AX_Y, AX_C))
    place, places = (z * ny + y) * nc + c, nz * ny * nc
    ring = Ring(t_buf, (ring_send, ring_recv))
    ins = [Torus(wa, AX_Y, 2, torus[0:6]), Torus(wb, AX_Z, 2, torus[6:12])]
    outs = [Torus(oa, AX_Y, 4, torus[12:18]), Torus(ob, AX_Z, 4, torus[18:24])]
    loads = [
        pltpu.make_async_copy(tok_ref, t_buf.at[x], load_sem.at[0]),
        pltpu.make_async_copy(q_ref, wa.at[z, y, c], load_sem.at[1]),
        pltpu.make_async_copy(k_ref, wb.at[z, y, c, :, 0:128], load_sem.at[2]),
        pltpu.make_async_copy(v_ref, wb.at[z, y, c, :, 128:256], load_sem.at[3]),
        pltpu.make_async_copy(p_ref, wb.at[z, y, c, :, 256:512], load_sem.at[4]),
        pltpu.make_async_copy(oa_ref, oa.at[z, y, c], load_sem.at[5]),
        pltpu.make_async_copy(ob_ref, ob.at[z, y, c], load_sem.at[6]),
    ]
    for load in loads:
        load.start()
    greet_all()
    for load in loads:
        load.wait()
    for t in ins:
        t.phase1_start()
    ring.start()
    for k in range(ins[0].groups):
        for t in ins:
            t.phase1_group(k)

    def levels(group, hop):
        for k in range(group[0].groups):
            for way in range(2):
                for t in group:
                    t.level(hop, k, way)

    levels(ins, 2)
    ring.forward()
    levels(ins, 3)
    levels(ins, 4)
    for t in outs:
        t.phase1_start()
    levels(ins, 5)
    ring.arrived()
    normalise(t_buf, gain_ref, normed)
    for k in range(outs[0].groups):
        for t in outs:
            t.phase1_group(k)
    for t in ins:
        t.arrived()

    project_keys(normed, wb, cos_ref, sin_ref, kv_ext)
    project_pool(normed, wb, pool_ext)

    def halo_copies(way):
        low = 512 if way == 0 else BLOCK
        high = 0 if way == 0 else BLOCK + 512
        plow = 512 if way == 0 else EDGE
        phigh = 0 if way == 0 else EDGE + 512
        device = sequence_neighbour(1 if way == 0 else -1)
        return [
            remote(
                kv_ext.at[low : low + BLOCK], kv_ext.at[high : high + BLOCK],
                halo_send.at[way, 0], halo_recv.at[way, 0], device,
            ),
            remote(
                pool_ext.at[plow : plow + EDGE], pool_ext.at[phigh : phigh + EDGE],
                halo_send.at[way, 1], halo_recv.at[way, 1], device,
            ),
        ]

    for way in range(2):
        for copy in halo_copies(way):
            copy.start()
    levels(outs, 2)
    for h in range(2):
        project_queries(normed, wa, cos_ref, sin_ref, queries, h)
    levels(outs, 3)
    reach = lax.shift_left(jnp.int32(1), x)

    def block(i, carry):
        b = i + 1 - 4 * lax.div(i, 3)
        for h in range(2):
            attend(b, h, place, places, kv_ext, queries, sink_ref, features, log_ref)
        pool(b, place, places, reach, pool_ext, mix_ref, features)
        return carry

    lax.fori_loop(0, 2, block, 0)
    levels(outs, 4)
    for way in range(2):
        for copy in halo_copies(way):
            copy.wait_recv()
    lax.fori_loop(2, 4, block, 0)
    levels(outs, 5)
    for t in outs:
        t.arrived()

    scatter = Scatter(
        (far, near, far_in, near_in, kept), (far_send, far_recv, near_send, near_recv)
    )

    def send(b, carry):
        scatter.compute(b, features, oa, ob)

        @pl.when(b > 0)
        def _():
            scatter.add(b - 1)

        return carry

    lax.fori_loop(0, 4, send, 0)
    scatter.add(3)

    def close(b, carry):
        scatter.finish(b, out_ref)
        scatter.drain(b)
        return carry

    lax.fori_loop(0, 4, close, 0)
    for t in ins + outs:
        t.drain()
    ring.drain()
    for way in range(2):
        for copy in halo_copies(way):
            copy.wait_send()


def whole_layer(tokens, weights, out_a, out_b, gain, mix, sink, cosine, sine):
    nz, ny, nc, nx = (lax.axis_size(a) for a in (AX_Z, AX_Y, AX_C, AX_X))
    rows, width = tokens.shape
    bf = jnp.bfloat16
    dma = pltpu.SemaphoreType.DMA
    vmem = pltpu.VMEM
    blocks = rows // BLOCK
    near_data = pl.BlockSpec(memory_space=pltpu.VMEM)
    return pl.pallas_call(
        layer_kernel,
        out_shape=[
            jax.ShapeDtypeStruct((rows, width), bf),
            jax.ShapeDtypeStruct((8, rows), jnp.float32),
        ],
        in_specs=[pl.BlockSpec(memory_space=pltpu.HBM)] * 7 + [near_data] * 5,
        out_specs=[near_data] * 2,
        scratch_shapes=[
            vmem((nx, rows, width), bf),
            vmem((nz, ny, nc, 16, 512), bf),
            vmem((nz, ny, nc, 16, 512), bf),
            vmem((nz, ny, nc, 16, 384), bf),
            vmem((nz, ny, nc, 16, 384), bf),
            vmem((rows, nx * width), bf),
            vmem((2, blocks, 4 * BLOCK, 128), bf),
            vmem((rows + 2 * BLOCK, 256), bf),
            vmem((rows + 2 * EDGE, 256), bf),
            vmem((rows, 768), bf),
            vmem((blocks, BLOCK, 512), bf),
            vmem((blocks, 2, BLOCK, 512), bf),
            vmem((blocks, 2, BLOCK // 2, 512), bf),
            vmem((blocks, 2, BLOCK, 512), bf),
            vmem((blocks, BLOCK, 512), bf),
            dma((7,)), dma((2, 3)), dma((2, 3)), dma((2, 2)), dma((2, 2)),
            dma((blocks, 2)), dma((blocks, 2)), dma((blocks, 2, 2)), dma((blocks, 2, 2)),
        ]
        + torus_sems(ny, nz, 2) + torus_sems(nz, ny, 2) + torus_sems(ny, nz, 4) + torus_sems(nz, ny, 4),
        compiler_params=pltpu.CompilerParams(
            collective_id=0, has_side_effects=True, vmem_limit_bytes=56 * 1024 * 1024
        ),
    )(tokens, *weights, out_a, out_b, gain, mix, sink, cosine, sine)


def local(
    tokens,
    norm_gain,
    query_weight,
    key_weight,
    value_weight,
    pool_in_weight,
    pool_mix_weight,
    sink_logit,
    out_pool_weight,
    out_attn_weight,
):
    rows = tokens.shape[0]
    positions = lax.axis_index(SP) * rows + jnp.arange(rows, dtype=jnp.int32)
    cos_r, sin_r, cos_c, sin_c = rope_tables(positions, HD)
    cosine = jnp.concatenate([cos_r, cos_r, cos_c, cos_c] * 2, 1)
    sine = jnp.concatenate([-sin_r, sin_r, -sin_c, sin_c] * 2, 1)
    out_rows = jnp.concatenate([out_pool_weight, out_attn_weight], 0).T
    mixed, log_weight = whole_layer(
        tokens,
        (query_weight, key_weight, value_weight, pool_in_weight),
        out_rows[:, :384],
        out_rows[:, 384:],
        norm_gain[None],
        pool_mix_weight,
        jnp.repeat(sink_logit, BLOCK).reshape(2, 4 * BLOCK),
        cosine,
        sine,
    )
    return (mixed, log_weight)


def solution(mesh):
    finer = Mesh(mesh.devices.reshape(8, 8, 2, mesh.shape["tp"]), ("sp_0", "sp_1", "sp_2", "tp"))
    placed = (
        P(SP, "tp"),
        P(),
        P(SP, "tp"),
        P(SP, "tp"),
        P(SP, "tp"),
        P(SP, "tp"),
        P("tp", None, None),
        P("tp"),
        P("tp", SP),
        P("tp", SP),
    )
    return jax.shard_map(
        local, mesh=finer, in_specs=placed, out_specs=(P(SP, "tp"), P("tp", SP)), check_vma=False
    )
```

```python
import jax
import jax.numpy as jnp
import numpy as np
from jax import lax
from jax.sharding import Mesh
from jax.experimental import pallas as pl
from jax.experimental.pallas import tpu as pltpu
from jax.sharding import PartitionSpec as P

HD = 64
GRID_W = 64
SP = ("sp_0", "sp_1", "sp_2")


norm_eps = 1e-06
rope_base = 10000.0
neg_fill = -1e30


MESH = pl.DeviceIdType.MESH
AX_Z, AX_Y, AX_C, AX_X = "sp_0", "sp_1", "sp_2", "tp"
BLOCK = 128
EDGE = 16


def remote(src, dst, send_sem, recv_sem, device):
    return pltpu.make_async_remote_copy(
        src_ref=src,
        dst_ref=dst,
        send_sem=send_sem,
        recv_sem=recv_sem,
        device_id=device,
        device_id_type=MESH,
    )


def wait_bytes(ref, sem):
    pltpu.make_async_copy(ref, ref, sem).wait()


class Torus:
    def __init__(self, buf, first, size, sems):
        self.buf, self.first, self.size = buf, first, size
        self.p1_send, self.p1_recv, self.p2_send, self.p2_recv, self.d_send, self.d_recv = sems
        self.z, self.y, self.c = lax.axis_index(AX_Z), lax.axis_index(AX_Y), lax.axis_index(AX_C)
        by_y = first == AX_Y
        self.n1, self.n2 = (buf.shape[1], buf.shape[0]) if by_y else (buf.shape[0], buf.shape[1])
        self.a, self.b = (self.y, self.z) if by_y else (self.z, self.y)
        self.second = AX_Z if by_y else AX_Y
        self.groups = self.n1 // size

    def chunk(self, b, start, size):
        if self.first == AX_Y:
            return self.buf.at[b, pl.ds(start, size), self.c]
        return self.buf.at[pl.ds(start, size), b, self.c]

    def group_id(self, k):
        return lax.rem(lax.div(self.a, self.size) + k, self.groups)

    def hops(self, way, k):
        half = self.n2 // 2
        return half if (way == 0) == (k < self.groups // 2) else half - 1

    def phase1_start(self):
        own = self.buf.at[self.z, self.y, self.c]
        order = sorted(range(1, self.n1), key=lambda d: min(d, self.n1 - d))
        for d in order:
            remote(
                own, own, self.p1_send, self.p1_recv.at[self.group_id(0)],
                {self.first: lax.rem(self.a + d, self.n1)},
            ).start()

    def to_partner(self, ref):
        remote(ref, ref, self.d_send, self.d_recv, {AX_C: 1 - self.c}).start()

    def phase1_group(self, k):
        count = self.size - 1 if k == 0 else self.size
        wait_bytes(self.chunk(self.b, 0, count), self.p1_recv.at[self.group_id(k)])
        for way in range(2):
            self.relay(way, k, 1).start()
        self.to_partner(self.chunk(self.b, self.group_id(k) * self.size, self.size))

    def block(self, way, k, back):
        step = 1 if way == 0 else self.n2 - 1
        origin = lax.rem(self.b + back * (self.n2 - step), self.n2)
        return self.chunk(origin, self.group_id(k) * self.size, self.size)

    def relay(self, way, k, hop):
        step = 1 if way == 0 else self.n2 - 1
        ref = self.block(way, k, hop - 1)
        return remote(
            ref, ref, self.p2_send.at[way, k, hop - 1], self.p2_recv.at[way, k, hop - 1],
            {self.second: lax.rem(self.b + step, self.n2)},
        )

    def level(self, hop, k, way):
        last = self.hops(way, k)
        if hop > last + 1:
            return
        ref = self.block(way, k, hop - 1)
        wait_bytes(ref, self.p2_recv.at[way, k, hop - 2])
        if hop <= last:
            self.relay(way, k, hop).start()
        self.to_partner(ref)

    def arrived(self):
        wait_bytes(self.buf.at[:, :, 1 - self.c], self.d_recv)

    def drain(self):
        wait_bytes(self.buf.at[:, :, self.c], self.d_send)
        wait_bytes(self.chunk(self.b, 0, self.n1 - 1), self.p1_send)
        for k in range(self.groups):
            for way in range(2):
                for hop in range(1, self.hops(way, k) + 1):
                    self.relay(way, k, hop).wait_send()


def torus_sems(n1, n2, size):
    dma = pltpu.SemaphoreType.DMA
    groups, hops = n1 // size, n2 // 2
    return [
        dma(()), dma((groups,)), dma((2, groups, hops)), dma((2, groups, hops)), dma(()), dma(()),
    ]


class Ring:
    def __init__(self, buf, sems):
        self.buf = buf
        self.send, self.recv = sems
        self.n, self.x = buf.shape[0], lax.axis_index(AX_X)
        self.half = buf.shape[1] // 2

    def part(self, x, which):
        return self.buf.at[x, which * self.half : (which + 1) * self.half]

    def copy(self, way, index, x, which):
        step = 1 if way == 0 else self.n - 1
        ref = self.part(x, which)
        return remote(
            ref, ref, self.send.at[way, index], self.recv.at[way, index],
            {AX_X: lax.rem(self.x + step, self.n)},
        )

    def start(self):
        for index in range(2):
            for way in range(2):
                self.copy(way, index, self.x, index if way == 0 else 1 - index).start()

    def forward(self):
        for way in range(2):
            step = 1 if way == 0 else self.n - 1
            behind = lax.rem(self.x + self.n - step, self.n)
            wait_bytes(self.part(behind, way), self.recv.at[way, 0])
            self.copy(way, 2, behind, way).start()

    def arrived(self):
        for way in range(2):
            step = 1 if way == 0 else self.n - 1
            behind = lax.rem(self.x + self.n - step, self.n)
            across = lax.rem(self.x + 2, self.n)
            wait_bytes(self.part(behind, 1 - way), self.recv.at[way, 1])
            wait_bytes(self.part(across, way), self.recv.at[way, 2])

    def drain(self):
        for way in range(2):
            for index in range(3):
                self.copy(way, index, self.x, 0).wait_send()


def sequence_neighbour(step):
    nz, ny, nc = (lax.axis_size(a) for a in (AX_Z, AX_Y, AX_C))
    place = (lax.axis_index(AX_Z) * ny + lax.axis_index(AX_Y)) * nc + lax.axis_index(AX_C)
    place = lax.rem(place + step + nz * ny * nc, nz * ny * nc)
    chip = lax.div(place, nc)
    return {AX_Z: lax.div(chip, ny), AX_Y: lax.rem(chip, ny), AX_C: lax.rem(place, nc)}


def greet_all():
    nz, ny, nx = (lax.axis_size(a) for a in (AX_Z, AX_Y, AX_X))
    z, y, c, x = (lax.axis_index(a) for a in (AX_Z, AX_Y, AX_C, AX_X))
    peers = [sequence_neighbour(1), sequence_neighbour(-1), {AX_C: 1 - c}]
    peers += [{AX_X: lax.rem(x + d, nx)} for d in (1, nx - 1)]
    peers += [{AX_Y: lax.rem(y + d, ny)} for d in range(1, ny)]
    peers += [{AX_Z: lax.rem(z + d, nz)} for d in range(1, nz)]
    barrier = pltpu.get_barrier_semaphore()
    for peer in peers:
        pl.semaphore_signal(barrier, inc=1, device_id=peer, device_id_type=MESH)
    pl.semaphore_wait(barrier, len(peers))


def turned(values, cosine, sine):
    lane = lax.broadcasted_iota(jnp.int32, values.shape, 1)
    ahead = pltpu.roll(values, 112, 1)
    behind = pltpu.roll(values, 16, 1)
    return values * cosine + jnp.where(lax.rem(lane, 32) < 16, ahead, behind) * sine


def rounded(values):
    return values.astype(jnp.bfloat16).astype(jnp.float32)


def fill_tables(place, freq_ref, cos_buf, sin_buf):
    row = (lax.broadcasted_iota(jnp.int32, (8, 128), 0) + place * 8).astype(jnp.float32)
    row_cos, row_sin = jnp.cos(row * freq_ref[0:1]), jnp.sin(row * freq_ref[0:1])
    col = lax.broadcasted_iota(jnp.int32, (GRID_W, 128), 0).astype(jnp.float32)
    col_cos, col_sin = jnp.cos(col * freq_ref[0:1]), jnp.sin(col * freq_ref[0:1])
    lane = lax.broadcasted_iota(jnp.int32, (GRID_W, 128), 1)
    by_row = lax.rem(lane, 64) < 32
    sign = jnp.where(lax.rem(lane, 32) < 16, -1.0, 1.0)
    for r in range(8):
        rows = slice(r * GRID_W, (r + 1) * GRID_W)
        cos_buf[rows] = jnp.where(by_row, row_cos[r : r + 1], col_cos)
        sin_buf[rows] = jnp.where(by_row, row_sin[r : r + 1], col_sin) * sign


def rows_of(buf, start, size, columns):
    parts = buf[start // 256 : (start + size) // 256, :, :, :, columns]
    return parts.reshape(size, -1)


def normalise(t_buf, gain_ref, normed):
    def step(i, carry):
        rows = pl.ds(pl.multiple_of(i * BLOCK, BLOCK), BLOCK)
        parts = [t_buf[k, rows, :].astype(jnp.float32) for k in range(4)]
        total = sum(jnp.sum(p * p, axis=-1, keepdims=True) for p in parts)
        scale = lax.rsqrt(total / 2048.0 + norm_eps)
        for k in range(4):
            cols = slice(k * 512, (k + 1) * 512)
            normed[rows, cols] = (parts[k] * scale * gain_ref[0:1, cols]).astype(jnp.bfloat16)
        return carry

    lax.fori_loop(0, 4, step, 0)


def project_keys(normed, wb, cos_ref, sin_ref, kv_ext):
    both = jnp.dot(
        normed[...], rows_of(wb, 0, 2048, slice(0, 256)), preferred_element_type=jnp.float32
    )
    keys = turned(rounded(both[:, :128]), cos_ref[...], sin_ref[...])
    kv_ext[BLOCK : BLOCK + 512, 0:128] = keys.astype(jnp.bfloat16)
    kv_ext[BLOCK : BLOCK + 512, 128:256] = both[:, 128:].astype(jnp.bfloat16)


def project_pool(normed, wb, pool_ext):
    pool_ext[EDGE : EDGE + 512, :] = jnp.dot(
        normed[...], rows_of(wb, 0, 2048, slice(256, 512)), preferred_element_type=jnp.float32
    ).astype(jnp.bfloat16)


def project_queries(normed, wa, cos_ref, sin_ref, queries, h):
    cols = slice(h * 256, (h + 1) * 256)
    found = jnp.dot(normed[...], rows_of(wa, 0, 2048, cols), preferred_element_type=jnp.float32)
    for pair in range(2):
        values = turned(
            rounded(found[:, pair * 128 : (pair + 1) * 128]), cos_ref[...], sin_ref[...]
        ) * (HD**-0.5)
        lane = lax.broadcasted_iota(jnp.int32, values.shape, 1)
        mine = (lane < 64) if h == 0 else (lane >= 64)
        for odd in range(2):
            placed = values if odd == h else pltpu.roll(values, 64, 1)
            placed = jnp.where(mine, placed, 0.0).astype(jnp.bfloat16)
            g = pair * 2 + odd
            for b in range(4):
                queries[h, b, g * BLOCK : (g + 1) * BLOCK, :] = placed[b * BLOCK : (b + 1) * BLOCK]


def attend(b, h, place, places, kv_ext, queries, sink_ref, features, log_ref):
    start = pl.multiple_of(b * BLOCK, BLOCK)
    keys = kv_ext[pl.ds(start, 3 * BLOCK), 0:128]
    scores = lax.dot_general(
        keys, queries[h, b], (((1,), (1,)), ((), ())), preferred_element_type=jnp.float32
    )
    shape = (BLOCK, 4 * BLOCK)
    key = lax.broadcasted_iota(jnp.int32, shape, 0)
    query = lax.rem(lax.broadcasted_iota(jnp.int32, shape, 1), BLOCK)
    first = jnp.where((place == 0) & (b == 0), BLOCK, 0)
    last = jnp.where((place == places - 1) & (b == 3), -1, BLOCK)
    before = jnp.where(key >= jnp.maximum(query, first), scores[:BLOCK], neg_fill)
    here = scores[BLOCK : 2 * BLOCK]
    after = jnp.where(key <= jnp.minimum(query, last), scores[2 * BLOCK :], neg_fill)
    sink = jnp.concatenate([jnp.full((1, BLOCK), sink_ref[4 * h + g], jnp.float32) for g in range(4)], 1)
    top = jnp.max(jnp.maximum(jnp.maximum(before, here), after), axis=0, keepdims=True)
    top = jnp.maximum(top, sink)
    exps = [jnp.exp(part - top) for part in (before, here, after)]
    total = jnp.sum(exps[0] + exps[1] + exps[2], axis=0, keepdims=True) + jnp.exp(sink - top)
    logs = top + jnp.log(total)
    weights = jnp.concatenate([e.astype(jnp.bfloat16) for e in exps], axis=0)
    values = kv_ext[pl.ds(start, 3 * BLOCK), 128:256]
    summed = lax.dot_general(
        values, weights, (((0,), (0,)), ((), ())), preferred_element_type=jnp.float32
    )
    mine = summed[h * 64 : (h + 1) * 64] / total
    for g in range(4):
        log_ref[4 * h + g : 4 * h + g + 1, pl.ds(start, BLOCK)] = logs[
            :, g * BLOCK : (g + 1) * BLOCK
        ]
    for pair in range(2):
        two = jnp.concatenate(
            [mine[:, (2 * pair + e) * BLOCK : (2 * pair + e + 1) * BLOCK] for e in range(2)], axis=0
        )
        at = 256 + h * 256 + pair * 128
        features[pl.ds(start, BLOCK), at : at + 128] = two.T.astype(jnp.bfloat16)


def pool(b, place, places, reach, pool_ext, mix_ref, features):
    start = pl.multiple_of(b * BLOCK, BLOCK)
    size = BLOCK + 2 * EDGE
    base = place * 512 + b * BLOCK
    row = lax.broadcasted_iota(jnp.int32, (BLOCK, size), 0)
    col = lax.broadcasted_iota(jnp.int32, (BLOCK, size), 1) - EDGE
    inside = (col >= row - reach) & (col < row + reach)
    inside = inside & (col >= -base) & (col < places * 512 - base)
    band = jnp.where(inside, 1.0, 0.0)
    counted = jnp.sum(band, axis=-1, keepdims=True)
    ext = pool_ext[pl.ds(start, size), :]
    summed = jnp.dot(band.astype(jnp.bfloat16), ext, preferred_element_type=jnp.float32)
    own = ext[EDGE : EDGE + BLOCK].astype(jnp.float32)
    pooled = (summed / counted - own).astype(jnp.bfloat16)
    features[pl.ds(start, BLOCK), 0:256] = jnp.dot(
        pooled, mix_ref[0], preferred_element_type=jnp.float32
    ).astype(jnp.bfloat16)


def partial_term(b, j, features, oa, ob):
    rows = pl.ds(pl.multiple_of(b * BLOCK, BLOCK), BLOCK)
    dims = (((1,), (1,)), ((), ()))
    low = oa[pl.ds(2 * j, 2)].reshape(512, 384)
    high = ob[pl.ds(2 * j, 2)].reshape(512, 384)
    return lax.dot_general(
        features[rows, 0:384], low, dims, preferred_element_type=jnp.float32
    ) + lax.dot_general(features[rows, 384:768], high, dims, preferred_element_type=jnp.float32)


class Scatter:
    def __init__(self, refs, sems):
        self.far, self.near, self.far_in, self.near_in, self.kept = refs
        self.far_send, self.far_recv, self.near_send, self.near_recv = sems
        self.n, self.x = lax.axis_size(AX_X), lax.axis_index(AX_X)
        self.half = BLOCK // 2

    def target(self, way):
        return lax.rem(self.x + (1 if way == 0 else self.n - 1), self.n)

    def far_copy(self, b, way):
        rows = slice(way * self.half, (way + 1) * self.half)
        return remote(
            self.far.at[b, rows], self.far_in.at[b, way],
            self.far_send.at[b, way], self.far_recv.at[b, way], {AX_X: self.target(way)},
        )

    def near_copy(self, b, way, added):
        which = way if added else 1 - way
        rows = slice(which * self.half, (which + 1) * self.half)
        index = 1 if added else 0
        return remote(
            self.near.at[b, way, rows], self.near_in.at[b, way, rows],
            self.near_send.at[b, way, index], self.near_recv.at[b, way, index],
            {AX_X: self.target(way)},
        )

    def compute(self, b, features, oa, ob):
        across = lax.rem(self.x + 2, self.n)
        self.far[b] = partial_term(b, across, features, oa, ob).astype(jnp.bfloat16)
        for way in range(2):
            self.near[b, way] = partial_term(b, self.target(way), features, oa, ob).astype(jnp.bfloat16)
            self.far_copy(b, way).start()
        self.kept[b] = partial_term(b, self.x, features, oa, ob).astype(jnp.bfloat16)
        for way in range(2):
            self.near_copy(b, way, False).start()

    def add(self, b):
        for way in range(2):
            rows = slice(way * self.half, (way + 1) * self.half)
            self.far_copy(b, way).wait_recv()
            both = self.near[b, way, rows].astype(jnp.float32) + self.far_in[b, way].astype(jnp.float32)
            self.near[b, way, rows] = both.astype(jnp.bfloat16)
        for way in range(2):
            self.near_copy(b, way, True).start()

    def finish(self, b, out_ref):
        for way in range(2):
            for added in (False, True):
                self.near_copy(b, way, added).wait_recv()
        total = self.kept[b].astype(jnp.float32)
        for way in range(2):
            total = total + self.near_in[b, way].astype(jnp.float32)
        out_ref[pl.ds(pl.multiple_of(b * BLOCK, BLOCK), BLOCK), :] = total.astype(jnp.bfloat16)

    def drain(self, b):
        for way in range(2):
            self.far_copy(b, way).wait_send()
            for added in (False, True):
                self.near_copy(b, way, added).wait_send()


def layer_kernel(
    tok_ref, q_ref, k_ref, v_ref, p_ref, op_ref, oq_ref,
    gain_ref, mix_ref, freq_ref, sink_ref,
    out_ref, log_ref,
    t_buf, wa, wb, oa, ob, cos_ref, sin_ref, normed, queries, kv_ext, pool_ext, features,
    far, near, far_in, near_in, kept,
    load_sem, ring_send, ring_recv, halo_send, halo_recv, far_send, far_recv, near_send, near_recv,
    *torus,
):
    z, y, c, x = (lax.axis_index(a) for a in (AX_Z, AX_Y, AX_C, AX_X))
    nz, ny, nc = (lax.axis_size(a) for a in (AX_Z, AX_Y, AX_C))
    place, places = (z * ny + y) * nc + c, nz * ny * nc
    ring = Ring(t_buf, (ring_send, ring_recv))
    ins = [Torus(wa, AX_Y, 2, torus[0:6]), Torus(wb, AX_Z, 2, torus[6:12])]
    outs = [Torus(oa, AX_Y, 4, torus[12:18]), Torus(ob, AX_Z, 4, torus[18:24])]
    loads = [
        pltpu.make_async_copy(tok_ref, t_buf.at[x], load_sem.at[0]),
        pltpu.make_async_copy(q_ref, wa.at[z, y, c], load_sem.at[1]),
        pltpu.make_async_copy(k_ref, wb.at[z, y, c, :, 0:128], load_sem.at[2]),
        pltpu.make_async_copy(v_ref, wb.at[z, y, c, :, 128:256], load_sem.at[3]),
        pltpu.make_async_copy(p_ref, wb.at[z, y, c, :, 256:512], load_sem.at[4]),
        pltpu.make_async_copy(op_ref, oa.at[z, y, c, :, 0:256], load_sem.at[5]),
        pltpu.make_async_copy(oq_ref.at[:, 0:128], oa.at[z, y, c, :, 256:384], load_sem.at[6]),
        pltpu.make_async_copy(oq_ref.at[:, 128:512], ob.at[z, y, c], load_sem.at[7]),
    ]
    for load in loads:
        load.start()
    greet_all()
    for load in loads:
        load.wait()
    for t in ins:
        t.phase1_start()
    ring.start()
    fill_tables(place, freq_ref, cos_ref, sin_ref)

    def first(group, k):
        for t in group:
            t.phase1_group(k)

    def levels(group, hop):
        for k in range(group[0].groups):
            for way in range(2):
                for t in group:
                    t.level(hop, k, way)

    for k in range(ins[0].groups):
        first(ins, k)
    for t in outs:
        t.phase1_start()
    levels(ins, 2)
    ring.forward()
    levels(ins, 3)
    for k in range(outs[0].groups):
        first(outs, k)
    levels(ins, 4)
    levels(outs, 2)
    levels(ins, 5)
    ring.arrived()
    levels(outs, 3)
    normalise(t_buf, gain_ref, normed)
    for t in ins:
        t.arrived()

    project_keys(normed, wb, cos_ref, sin_ref, kv_ext)
    project_pool(normed, wb, pool_ext)

    def halo_copies(way):
        low = 512 if way == 0 else BLOCK
        high = 0 if way == 0 else BLOCK + 512
        plow = 512 if way == 0 else EDGE
        phigh = 0 if way == 0 else EDGE + 512
        device = sequence_neighbour(1 if way == 0 else -1)
        return [
            remote(
                kv_ext.at[low : low + BLOCK], kv_ext.at[high : high + BLOCK],
                halo_send.at[way, 0], halo_recv.at[way, 0], device,
            ),
            remote(
                pool_ext.at[plow : plow + EDGE], pool_ext.at[phigh : phigh + EDGE],
                halo_send.at[way, 1], halo_recv.at[way, 1], device,
            ),
        ]

    for way in range(2):
        for copy in halo_copies(way):
            copy.start()
    for h in range(2):
        project_queries(normed, wa, cos_ref, sin_ref, queries, h)
    levels(outs, 4)
    levels(outs, 5)
    for t in outs:
        t.arrived()
    reach = lax.shift_left(jnp.int32(1), x)
    scatter = Scatter(
        (far, near, far_in, near_in, kept), (far_send, far_recv, near_send, near_recv)
    )

    def block(i, carry):
        b = lax.rem(i + 1, 4)
        for h in range(2):
            attend(b, h, place, places, kv_ext, queries, sink_ref, features, log_ref)
        pool(b, place, places, reach, pool_ext, mix_ref, features)
        scatter.compute(b, features, oa, ob)

        @pl.when(i > 0)
        def _():
            scatter.add(i)

        return carry

    lax.fori_loop(0, 2, block, 0)
    for way in range(2):
        for copy in halo_copies(way):
            copy.wait_recv()
    lax.fori_loop(2, 4, block, 0)
    scatter.add(0)

    def close(i, carry):
        b = lax.rem(i + 1, 4)
        scatter.finish(b, out_ref)
        scatter.drain(b)
        return carry

    lax.fori_loop(0, 4, close, 0)
    for t in ins + outs:
        t.drain()
    ring.drain()
    for way in range(2):
        for copy in halo_copies(way):
            copy.wait_send()


def whole_layer(tokens, weights, gain, mix, freq, sink):
    nz, ny, nc, nx = (lax.axis_size(a) for a in (AX_Z, AX_Y, AX_C, AX_X))
    rows, width = tokens.shape
    bf = jnp.bfloat16
    dma = pltpu.SemaphoreType.DMA
    vmem = pltpu.VMEM
    blocks = rows // BLOCK
    near_data = pl.BlockSpec(memory_space=pltpu.VMEM)
    return pl.pallas_call(
        layer_kernel,
        out_shape=[
            jax.ShapeDtypeStruct((rows, width), bf),
            jax.ShapeDtypeStruct((8, rows), jnp.float32),
        ],
        in_specs=[pl.BlockSpec(memory_space=pltpu.HBM)] * 7 + [near_data] * 3
        + [pl.BlockSpec(memory_space=pltpu.SMEM)],
        out_specs=[near_data] * 2,
        scratch_shapes=[
            vmem((nx, rows, width), bf),
            vmem((nz, ny, nc, 16, 512), bf),
            vmem((nz, ny, nc, 16, 512), bf),
            vmem((nz, ny, nc, 16, 384), bf),
            vmem((nz, ny, nc, 16, 384), bf),
            vmem((rows, 128), jnp.float32),
            vmem((rows, 128), jnp.float32),
            vmem((rows, nx * width), bf),
            vmem((2, blocks, 4 * BLOCK, 128), bf),
            vmem((rows + 2 * BLOCK, 256), bf),
            vmem((rows + 2 * EDGE, 256), bf),
            vmem((rows, 768), bf),
            vmem((blocks, BLOCK, 512), bf),
            vmem((blocks, 2, BLOCK, 512), bf),
            vmem((blocks, 2, BLOCK // 2, 512), bf),
            vmem((blocks, 2, BLOCK, 512), bf),
            vmem((blocks, BLOCK, 512), bf),
            dma((8,)), dma((2, 3)), dma((2, 3)), dma((2, 2)), dma((2, 2)),
            dma((blocks, 2)), dma((blocks, 2)), dma((blocks, 2, 2)), dma((blocks, 2, 2)),
        ]
        + torus_sems(ny, nz, 2) + torus_sems(nz, ny, 2) + torus_sems(ny, nz, 4) + torus_sems(nz, ny, 4),
        compiler_params=pltpu.CompilerParams(
            collective_id=0, has_side_effects=True, vmem_limit_bytes=56 * 1024 * 1024
        ),
    )(tokens, *weights, gain, mix, freq, sink)


def local(
    tokens,
    norm_gain,
    query_weight,
    key_weight,
    value_weight,
    pool_in_weight,
    pool_mix_weight,
    sink_logit,
    out_pool_weight,
    out_attn_weight,
):
    lane = np.arange(128)
    freq = (rope_base ** (-(lane % 16) / 16.0)).astype(np.float32)[None]
    mixed, log_weight = whole_layer(
        tokens,
        (query_weight, key_weight, value_weight, pool_in_weight, out_pool_weight.T, out_attn_weight.T),
        norm_gain[None],
        pool_mix_weight,
        jnp.asarray(freq),
        sink_logit,
    )
    return (mixed, log_weight)


def solution(mesh):
    finer = Mesh(mesh.devices.reshape(8, 8, 2, mesh.shape["tp"]), ("sp_0", "sp_1", "sp_2", "tp"))
    placed = (
        P(SP, "tp"),
        P(),
        P(SP, "tp"),
        P(SP, "tp"),
        P(SP, "tp"),
        P(SP, "tp"),
        P("tp", None, None),
        P("tp"),
        P("tp", SP),
        P("tp", SP),
    )
    return jax.shard_map(
        local, mesh=finer, in_specs=placed, out_specs=(P(SP, "tp"), P("tp", SP)), check_vma=False
    )
```

```python
import jax
import jax.numpy as jnp
import numpy as np
from jax import lax
from jax.sharding import Mesh
from jax.experimental import pallas as pl
from jax.experimental.pallas import tpu as pltpu
from jax.sharding import PartitionSpec as P

HD = 64
GRID_W = 64
SP = ("sp_0", "sp_1", "sp_2")


norm_eps = 1e-06
rope_base = 10000.0
neg_fill = -1e30


MESH = pl.DeviceIdType.MESH
AX_Z, AX_Y, AX_C, AX_X = "sp_0", "sp_1", "sp_2", "tp"
BLOCK = 128
EDGE = 16


def remote(src, dst, send_sem, recv_sem, device):
    return pltpu.make_async_remote_copy(
        src_ref=src,
        dst_ref=dst,
        send_sem=send_sem,
        recv_sem=recv_sem,
        device_id=device,
        device_id_type=MESH,
    )


def wait_bytes(ref, sem):
    pltpu.make_async_copy(ref, ref, sem).wait()


class Torus:
    def __init__(self, buf, first, size, sems):
        self.buf, self.first, self.size = buf, first, size
        self.p1_send, self.p1_recv, self.p2_send, self.p2_recv, self.d_send, self.d_recv = sems
        self.z, self.y, self.c = lax.axis_index(AX_Z), lax.axis_index(AX_Y), lax.axis_index(AX_C)
        by_y = first == AX_Y
        self.n1, self.n2 = (buf.shape[1], buf.shape[0]) if by_y else (buf.shape[0], buf.shape[1])
        self.a, self.b = (self.y, self.z) if by_y else (self.z, self.y)
        self.second = AX_Z if by_y else AX_Y
        self.groups = self.n1 // size

    def chunk(self, b, start, size):
        if self.first == AX_Y:
            return self.buf.at[b, pl.ds(start, size), self.c]
        return self.buf.at[pl.ds(start, size), b, self.c]

    def group_id(self, k):
        return lax.rem(lax.div(self.a, self.size) + k, self.groups)

    def hops(self, way, k):
        half = self.n2 // 2
        return half if (way == 0) == (k < self.groups // 2) else half - 1

    def phase1_start(self):
        own = self.buf.at[self.z, self.y, self.c]
        order = sorted(range(1, self.n1), key=lambda d: min(d, self.n1 - d))
        for d in order:
            remote(
                own, own, self.p1_send, self.p1_recv.at[self.group_id(0)],
                {self.first: lax.rem(self.a + d, self.n1)},
            ).start()

    def to_partner(self, ref):
        remote(ref, ref, self.d_send, self.d_recv, {AX_C: 1 - self.c}).start()

    def phase1_group(self, k):
        count = self.size - 1 if k == 0 else self.size
        wait_bytes(self.chunk(self.b, 0, count), self.p1_recv.at[self.group_id(k)])
        for way in range(2):
            self.relay(way, k, 1).start()

    def block(self, way, k, back):
        step = 1 if way == 0 else self.n2 - 1
        origin = lax.rem(self.b + back * (self.n2 - step), self.n2)
        return self.chunk(origin, self.group_id(k) * self.size, self.size)

    def relay(self, way, k, hop):
        step = 1 if way == 0 else self.n2 - 1
        ref = self.block(way, k, hop - 1)
        return remote(
            ref, ref, self.p2_send.at[way, k, hop - 1], self.p2_recv.at[way, k, hop - 1],
            {self.second: lax.rem(self.b + step, self.n2)},
        )

    def level(self, hop, k, way):
        last = self.hops(way, k)
        if hop > last + 1:
            return
        ref = self.block(way, k, hop - 1)
        wait_bytes(ref, self.p2_recv.at[way, k, hop - 2])
        if hop <= last:
            self.relay(way, k, hop).start()

    def share(self, back):
        for way in range(1 if 2 * back in (0, self.n2) else 2):
            step = 1 if way == 0 else self.n2 - 1
            origin = lax.rem(self.b + back * (self.n2 - step), self.n2)
            self.to_partner(self.chunk(origin, 0, self.n1))

    def arrived(self):
        wait_bytes(self.buf.at[:, :, 1 - self.c], self.d_recv)

    def drain(self):
        wait_bytes(self.buf.at[:, :, self.c], self.d_send)
        wait_bytes(self.chunk(self.b, 0, self.n1 - 1), self.p1_send)
        for k in range(self.groups):
            for way in range(2):
                for hop in range(1, self.hops(way, k) + 1):
                    self.relay(way, k, hop).wait_send()


def torus_sems(n1, n2, size):
    dma = pltpu.SemaphoreType.DMA
    groups, hops = n1 // size, n2 // 2
    return [
        dma(()), dma((groups,)), dma((2, groups, hops)), dma((2, groups, hops)), dma(()), dma(()),
    ]


class Ring:
    def __init__(self, buf, sems):
        self.buf = buf
        self.send, self.recv = sems
        self.n, self.x = buf.shape[0], lax.axis_index(AX_X)
        self.half = buf.shape[1] // 2

    def part(self, x, which):
        return self.buf.at[x, which * self.half : (which + 1) * self.half]

    def copy(self, way, index, x, which):
        step = 1 if way == 0 else self.n - 1
        ref = self.part(x, which)
        return remote(
            ref, ref, self.send.at[way, index], self.recv.at[way, index],
            {AX_X: lax.rem(self.x + step, self.n)},
        )

    def start(self):
        for index in range(2):
            for way in range(2):
                self.copy(way, index, self.x, index if way == 0 else 1 - index).start()

    def forward(self):
        for way in range(2):
            step = 1 if way == 0 else self.n - 1
            behind = lax.rem(self.x + self.n - step, self.n)
            wait_bytes(self.part(behind, way), self.recv.at[way, 0])
            self.copy(way, 2, behind, way).start()

    def arrived(self):
        for way in range(2):
            step = 1 if way == 0 else self.n - 1
            behind = lax.rem(self.x + self.n - step, self.n)
            across = lax.rem(self.x + 2, self.n)
            wait_bytes(self.part(behind, 1 - way), self.recv.at[way, 1])
            wait_bytes(self.part(across, way), self.recv.at[way, 2])

    def drain(self):
        for way in range(2):
            for index in range(3):
                self.copy(way, index, self.x, 0).wait_send()


def sequence_neighbour(step):
    nz, ny, nc = (lax.axis_size(a) for a in (AX_Z, AX_Y, AX_C))
    place = (lax.axis_index(AX_Z) * ny + lax.axis_index(AX_Y)) * nc + lax.axis_index(AX_C)
    place = lax.rem(place + step + nz * ny * nc, nz * ny * nc)
    chip = lax.div(place, nc)
    return {AX_Z: lax.div(chip, ny), AX_Y: lax.rem(chip, ny), AX_C: lax.rem(place, nc)}


def greet_all():
    nz, ny, nx = (lax.axis_size(a) for a in (AX_Z, AX_Y, AX_X))
    z, y, c, x = (lax.axis_index(a) for a in (AX_Z, AX_Y, AX_C, AX_X))
    peers = [sequence_neighbour(1), sequence_neighbour(-1), {AX_C: 1 - c}]
    peers += [{AX_X: lax.rem(x + d, nx)} for d in (1, nx - 1)]
    peers += [{AX_Y: lax.rem(y + d, ny)} for d in range(1, ny)]
    peers += [{AX_Z: lax.rem(z + d, nz)} for d in range(1, nz)]
    barrier = pltpu.get_barrier_semaphore()
    for peer in peers:
        pl.semaphore_signal(barrier, inc=1, device_id=peer, device_id_type=MESH)
    pl.semaphore_wait(barrier, len(peers))


def turned(values, cosine, sine):
    lane = lax.broadcasted_iota(jnp.int32, values.shape, 1)
    ahead = pltpu.roll(values, 112, 1)
    behind = pltpu.roll(values, 16, 1)
    return values * cosine + jnp.where(lax.rem(lane, 32) < 16, ahead, behind) * sine


def rounded(values):
    return values.astype(jnp.bfloat16).astype(jnp.float32)


def fill_tables(place, freq_ref, cos_buf, sin_buf):
    row = (lax.broadcasted_iota(jnp.int32, (8, 128), 0) + place * 8).astype(jnp.float32)
    row_cos, row_sin = jnp.cos(row * freq_ref[0:1]), jnp.sin(row * freq_ref[0:1])
    col = lax.broadcasted_iota(jnp.int32, (GRID_W, 128), 0).astype(jnp.float32)
    col_cos, col_sin = jnp.cos(col * freq_ref[0:1]), jnp.sin(col * freq_ref[0:1])
    lane = lax.broadcasted_iota(jnp.int32, (GRID_W, 128), 1)
    by_row = lax.rem(lane, 64) < 32
    sign = jnp.where(lax.rem(lane, 32) < 16, -1.0, 1.0)
    for r in range(8):
        rows = slice(r * GRID_W, (r + 1) * GRID_W)
        cos_buf[rows] = jnp.where(by_row, row_cos[r : r + 1], col_cos)
        sin_buf[rows] = jnp.where(by_row, row_sin[r : r + 1], col_sin) * sign


def rows_of(buf, start, size, columns):
    parts = buf[start // 256 : (start + size) // 256, :, :, :, columns]
    return parts.reshape(size, -1)


def normalise(t_buf, gain_ref, normed):
    def step(i, carry):
        rows = pl.ds(pl.multiple_of(i * BLOCK, BLOCK), BLOCK)
        parts = [t_buf[k, rows, :].astype(jnp.float32) for k in range(4)]
        total = sum(jnp.sum(p * p, axis=-1, keepdims=True) for p in parts)
        scale = lax.rsqrt(total / 2048.0 + norm_eps)
        for k in range(4):
            cols = slice(k * 512, (k + 1) * 512)
            normed[rows, cols] = (parts[k] * scale * gain_ref[0:1, cols]).astype(jnp.bfloat16)
        return carry

    lax.fori_loop(0, 4, step, 0)


def project_keys(normed, wb, cos_ref, sin_ref, kv_ext):
    both = jnp.dot(
        normed[...], rows_of(wb, 0, 2048, slice(0, 256)), preferred_element_type=jnp.float32
    )
    keys = turned(rounded(both[:, :128]), cos_ref[...], sin_ref[...])
    kv_ext[BLOCK : BLOCK + 512, 0:128] = keys.astype(jnp.bfloat16)
    kv_ext[BLOCK : BLOCK + 512, 128:256] = both[:, 128:].astype(jnp.bfloat16)


def project_pool(normed, wb, pool_ext):
    pool_ext[EDGE : EDGE + 512, :] = jnp.dot(
        normed[...], rows_of(wb, 0, 2048, slice(256, 512)), preferred_element_type=jnp.float32
    ).astype(jnp.bfloat16)


def project_queries(normed, wa, cos_ref, sin_ref, queries, h):
    cols = slice(h * 256, (h + 1) * 256)
    found = jnp.dot(normed[...], rows_of(wa, 0, 2048, cols), preferred_element_type=jnp.float32)
    for pair in range(2):
        values = turned(
            rounded(found[:, pair * 128 : (pair + 1) * 128]), cos_ref[...], sin_ref[...]
        ) * (HD**-0.5)
        lane = lax.broadcasted_iota(jnp.int32, values.shape, 1)
        mine = (lane < 64) if h == 0 else (lane >= 64)
        for odd in range(2):
            placed = values if odd == h else pltpu.roll(values, 64, 1)
            placed = jnp.where(mine, placed, 0.0).astype(jnp.bfloat16)
            g = pair * 2 + odd
            for b in range(4):
                queries[h, b, g * BLOCK : (g + 1) * BLOCK, :] = placed[b * BLOCK : (b + 1) * BLOCK]


def attend(b, h, place, places, kv_ext, queries, sink_ref, features, log_ref):
    start = pl.multiple_of(b * BLOCK, BLOCK)
    keys = kv_ext[pl.ds(start, 3 * BLOCK), 0:128]
    scores = lax.dot_general(
        keys, queries[h, b], (((1,), (1,)), ((), ())), preferred_element_type=jnp.float32
    )
    shape = (BLOCK, 4 * BLOCK)
    key = lax.broadcasted_iota(jnp.int32, shape, 0)
    query = lax.rem(lax.broadcasted_iota(jnp.int32, shape, 1), BLOCK)
    first = jnp.where((place == 0) & (b == 0), BLOCK, 0)
    last = jnp.where((place == places - 1) & (b == 3), -1, BLOCK)
    before = jnp.where(key >= jnp.maximum(query, first), scores[:BLOCK], neg_fill)
    here = scores[BLOCK : 2 * BLOCK]
    after = jnp.where(key <= jnp.minimum(query, last), scores[2 * BLOCK :], neg_fill)
    sink = jnp.concatenate([jnp.full((1, BLOCK), sink_ref[4 * h + g], jnp.float32) for g in range(4)], 1)
    top = jnp.max(jnp.maximum(jnp.maximum(before, here), after), axis=0, keepdims=True)
    top = jnp.maximum(top, sink)
    exps = [jnp.exp(part - top) for part in (before, here, after)]
    total = jnp.sum(exps[0] + exps[1] + exps[2], axis=0, keepdims=True) + jnp.exp(sink - top)
    logs = top + jnp.log(total)
    weights = jnp.concatenate([e.astype(jnp.bfloat16) for e in exps], axis=0)
    values = kv_ext[pl.ds(start, 3 * BLOCK), 128:256]
    summed = lax.dot_general(
        values, weights, (((0,), (0,)), ((), ())), preferred_element_type=jnp.float32
    )
    mine = summed[h * 64 : (h + 1) * 64] / total
    for g in range(4):
        log_ref[4 * h + g : 4 * h + g + 1, pl.ds(start, BLOCK)] = logs[
            :, g * BLOCK : (g + 1) * BLOCK
        ]
    for pair in range(2):
        two = jnp.concatenate(
            [mine[:, (2 * pair + e) * BLOCK : (2 * pair + e + 1) * BLOCK] for e in range(2)], axis=0
        )
        at = 256 + h * 256 + pair * 128
        features[pl.ds(start, BLOCK), at : at + 128] = two.T.astype(jnp.bfloat16)


def pool(b, place, places, reach, pool_ext, mix_ref, features):
    start = pl.multiple_of(b * BLOCK, BLOCK)
    size = BLOCK + 2 * EDGE
    base = place * 512 + b * BLOCK
    row = lax.broadcasted_iota(jnp.int32, (BLOCK, size), 0)
    col = lax.broadcasted_iota(jnp.int32, (BLOCK, size), 1) - EDGE
    inside = (col >= row - reach) & (col < row + reach)
    inside = inside & (col >= -base) & (col < places * 512 - base)
    band = jnp.where(inside, 1.0, 0.0)
    counted = jnp.sum(band, axis=-1, keepdims=True)
    ext = pool_ext[pl.ds(start, size), :]
    summed = jnp.dot(band.astype(jnp.bfloat16), ext, preferred_element_type=jnp.float32)
    own = ext[EDGE : EDGE + BLOCK].astype(jnp.float32)
    pooled = (summed / counted - own).astype(jnp.bfloat16)
    features[pl.ds(start, BLOCK), 0:256] = jnp.dot(
        pooled, mix_ref[0], preferred_element_type=jnp.float32
    ).astype(jnp.bfloat16)


def partial_term(b, j, features, oa, ob):
    rows = pl.ds(pl.multiple_of(b * BLOCK, BLOCK), BLOCK)
    dims = (((1,), (1,)), ((), ()))
    low = oa[pl.ds(2 * j, 2)].reshape(512, 384)
    high = ob[pl.ds(2 * j, 2)].reshape(512, 384)
    return lax.dot_general(
        features[rows, 0:384], low, dims, preferred_element_type=jnp.float32
    ) + lax.dot_general(features[rows, 384:768], high, dims, preferred_element_type=jnp.float32)


class Scatter:
    def __init__(self, refs, sems):
        self.far, self.near, self.far_in, self.near_in, self.kept = refs
        self.far_send, self.far_recv, self.near_send, self.near_recv = sems
        self.n, self.x = lax.axis_size(AX_X), lax.axis_index(AX_X)
        self.half = BLOCK // 2

    def target(self, way):
        return lax.rem(self.x + (1 if way == 0 else self.n - 1), self.n)

    def far_copy(self, b, way):
        rows = slice(way * self.half, (way + 1) * self.half)
        return remote(
            self.far.at[b, rows], self.far_in.at[b, way],
            self.far_send.at[b, way], self.far_recv.at[b, way], {AX_X: self.target(way)},
        )

    def near_copy(self, b, way, added):
        which = way if added else 1 - way
        rows = slice(which * self.half, (which + 1) * self.half)
        index = 1 if added else 0
        return remote(
            self.near.at[b, way, rows], self.near_in.at[b, way, rows],
            self.near_send.at[b, way, index], self.near_recv.at[b, way, index],
            {AX_X: self.target(way)},
        )

    def compute(self, b, features, oa, ob):
        across = lax.rem(self.x + 2, self.n)
        self.far[b] = partial_term(b, across, features, oa, ob).astype(jnp.bfloat16)
        for way in range(2):
            self.near[b, way] = partial_term(b, self.target(way), features, oa, ob).astype(jnp.bfloat16)
            self.far_copy(b, way).start()
        self.kept[b] = partial_term(b, self.x, features, oa, ob).astype(jnp.bfloat16)
        for way in range(2):
            self.near_copy(b, way, False).start()

    def add(self, b):
        for way in range(2):
            rows = slice(way * self.half, (way + 1) * self.half)
            self.far_copy(b, way).wait_recv()
            both = self.near[b, way, rows].astype(jnp.float32) + self.far_in[b, way].astype(jnp.float32)
            self.near[b, way, rows] = both.astype(jnp.bfloat16)
        for way in range(2):
            self.near_copy(b, way, True).start()

    def finish(self, b, out_ref):
        for way in range(2):
            for added in (False, True):
                self.near_copy(b, way, added).wait_recv()
        total = self.kept[b].astype(jnp.float32)
        for way in range(2):
            total = total + self.near_in[b, way].astype(jnp.float32)
        out_ref[pl.ds(pl.multiple_of(b * BLOCK, BLOCK), BLOCK), :] = total.astype(jnp.bfloat16)

    def drain(self, b):
        for way in range(2):
            self.far_copy(b, way).wait_send()
            for added in (False, True):
                self.near_copy(b, way, added).wait_send()


def layer_kernel(
    tok_ref, q_ref, k_ref, v_ref, p_ref, op_ref, oq_ref,
    gain_hbm, mix_hbm, freq_ref, sink_ref,
    out_ref, log_ref,
    t_buf, wa, wb, oa, ob, gain_ref, mix_ref, cos_ref, sin_ref, normed, queries, kv_ext, pool_ext, features,
    far, near, far_in, near_in, kept,
    load_sem, ring_send, ring_recv, halo_send, halo_recv, far_send, far_recv, near_send, near_recv,
    *torus,
):
    z, y, c, x = (lax.axis_index(a) for a in (AX_Z, AX_Y, AX_C, AX_X))
    nz, ny, nc = (lax.axis_size(a) for a in (AX_Z, AX_Y, AX_C))
    place, places = (z * ny + y) * nc + c, nz * ny * nc
    ring = Ring(t_buf, (ring_send, ring_recv))
    ins = [Torus(wa, AX_Y, 2, torus[0:6]), Torus(wb, AX_Z, 2, torus[6:12])]
    outs = [Torus(oa, AX_Y, 4, torus[12:18]), Torus(ob, AX_Z, 4, torus[18:24])]
    loads = [
        pltpu.make_async_copy(tok_ref, t_buf.at[x], load_sem.at[0]),
        pltpu.make_async_copy(q_ref, wa.at[z, y, c], load_sem.at[1]),
        pltpu.make_async_copy(k_ref, wb.at[z, y, c, :, 0:128], load_sem.at[2]),
        pltpu.make_async_copy(v_ref, wb.at[z, y, c, :, 128:256], load_sem.at[3]),
        pltpu.make_async_copy(p_ref, wb.at[z, y, c, :, 256:512], load_sem.at[4]),
        pltpu.make_async_copy(op_ref, oa.at[z, y, c, :, 0:256], load_sem.at[5]),
        pltpu.make_async_copy(oq_ref.at[:, 0:128], oa.at[z, y, c, :, 256:384], load_sem.at[6]),
        pltpu.make_async_copy(oq_ref.at[:, 128:512], ob.at[z, y, c], load_sem.at[7]),
    ]
    later = [
        pltpu.make_async_copy(gain_hbm, gain_ref, load_sem.at[8]),
        pltpu.make_async_copy(mix_hbm, mix_ref, load_sem.at[9]),
    ]
    for load in loads + later:
        load.start()
    greet_all()
    for load in loads:
        load.wait()
    for t in ins:
        t.phase1_start()
    ring.start()
    for load in later:
        load.wait()
    fill_tables(place, freq_ref, cos_ref, sin_ref)

    def first(group):
        for k in range(group[0].groups):
            for t in group:
                t.phase1_group(k)
        for t in group:
            t.share(0)

    def levels(group, hop):
        for k in range(group[0].groups):
            for way in range(2):
                for t in group:
                    t.level(hop, k, way)
        for t in group:
            t.share(hop - 1)


    def halo_copies(way):
        low = 512 if way == 0 else BLOCK
        high = 0 if way == 0 else BLOCK + 512
        plow = 512 if way == 0 else EDGE
        phigh = 0 if way == 0 else EDGE + 512
        device = sequence_neighbour(1 if way == 0 else -1)
        return [
            remote(
                kv_ext.at[low : low + BLOCK], kv_ext.at[high : high + BLOCK],
                halo_send.at[way, 0], halo_recv.at[way, 0], device,
            ),
            remote(
                pool_ext.at[plow : plow + EDGE], pool_ext.at[phigh : phigh + EDGE],
                halo_send.at[way, 1], halo_recv.at[way, 1], device,
            ),
        ]

    reach = lax.shift_left(jnp.int32(1), x)
    scatter = Scatter(
        (far, near, far_in, near_in, kept), (far_send, far_recv, near_send, near_recv)
    )

    def block(i, carry):
        b = lax.rem(i + 1, 4)
        for h in range(2):
            attend(b, h, place, places, kv_ext, queries, sink_ref, features, log_ref)
        pool(b, place, places, reach, pool_ext, mix_ref, features)
        return carry

    def send(i, carry):
        b = lax.rem(i + 1, 4)
        scatter.compute(b, features, oa, ob)

        @pl.when(i > 0)
        def _():
            scatter.add(i)

        return carry

    def both(i, carry):
        block(i, carry)
        return send(i, carry)

    for t in outs:
        t.phase1_start()
    first(ins)
    levels(ins, 2)
    ring.forward()
    first(outs)
    levels(ins, 3)
    levels(outs, 2)
    levels(ins, 4)
    levels(outs, 3)
    ring.arrived()
    normalise(t_buf, gain_ref, normed)
    levels(ins, 5)
    for t in ins:
        t.arrived()
    project_keys(normed, wb, cos_ref, sin_ref, kv_ext)
    project_pool(normed, wb, pool_ext)
    for way in range(2):
        for copy in halo_copies(way):
            copy.start()
    project_queries(normed, wa, cos_ref, sin_ref, queries, 0)
    levels(outs, 4)
    project_queries(normed, wa, cos_ref, sin_ref, queries, 1)
    block(0, 0)
    levels(outs, 5)
    for t in outs:
        t.arrived()
    send(0, 0)
    lax.fori_loop(1, 2, both, 0)
    for way in range(2):
        for copy in halo_copies(way):
            copy.wait_recv()
    lax.fori_loop(2, 4, both, 0)
    scatter.add(0)

    def close(i, carry):
        b = lax.rem(i + 1, 4)
        scatter.finish(b, out_ref)
        scatter.drain(b)
        return carry

    lax.fori_loop(0, 4, close, 0)
    for t in ins + outs:
        t.drain()
    ring.drain()
    for way in range(2):
        for copy in halo_copies(way):
            copy.wait_send()


def whole_layer(tokens, weights, gain, mix, freq, sink):
    nz, ny, nc, nx = (lax.axis_size(a) for a in (AX_Z, AX_Y, AX_C, AX_X))
    rows, width = tokens.shape
    bf = jnp.bfloat16
    dma = pltpu.SemaphoreType.DMA
    vmem = pltpu.VMEM
    blocks = rows // BLOCK
    near_data = pl.BlockSpec(memory_space=pltpu.VMEM)
    return pl.pallas_call(
        layer_kernel,
        out_shape=[
            jax.ShapeDtypeStruct((rows, width), bf),
            jax.ShapeDtypeStruct((8, rows), jnp.float32),
        ],
        in_specs=[pl.BlockSpec(memory_space=pltpu.HBM)] * 9 + [near_data]
        + [pl.BlockSpec(memory_space=pltpu.SMEM)],
        out_specs=[near_data] * 2,
        scratch_shapes=[
            vmem((nx, rows, width), bf),
            vmem((nz, ny, nc, 16, 512), bf),
            vmem((nz, ny, nc, 16, 512), bf),
            vmem((nz, ny, nc, 16, 384), bf),
            vmem((nz, ny, nc, 16, 384), bf),
            vmem((1, nx * width), jnp.float32),
            vmem((1, 256, 256), bf),
            vmem((rows, 128), jnp.float32),
            vmem((rows, 128), jnp.float32),
            vmem((rows, nx * width), bf),
            vmem((2, blocks, 4 * BLOCK, 128), bf),
            vmem((rows + 2 * BLOCK, 256), bf),
            vmem((rows + 2 * EDGE, 256), bf),
            vmem((rows, 768), bf),
            vmem((blocks, BLOCK, 512), bf),
            vmem((blocks, 2, BLOCK, 512), bf),
            vmem((blocks, 2, BLOCK // 2, 512), bf),
            vmem((blocks, 2, BLOCK, 512), bf),
            vmem((blocks, BLOCK, 512), bf),
            dma((10,)), dma((2, 3)), dma((2, 3)), dma((2, 2)), dma((2, 2)),
            dma((blocks, 2)), dma((blocks, 2)), dma((blocks, 2, 2)), dma((blocks, 2, 2)),
        ]
        + torus_sems(ny, nz, 2) + torus_sems(nz, ny, 2) + torus_sems(ny, nz, 4) + torus_sems(nz, ny, 4),
        compiler_params=pltpu.CompilerParams(
            collective_id=0, has_side_effects=True, vmem_limit_bytes=56 * 1024 * 1024
        ),
    )(tokens, *weights, gain, mix, freq, sink)


def local(
    tokens,
    norm_gain,
    query_weight,
    key_weight,
    value_weight,
    pool_in_weight,
    pool_mix_weight,
    sink_logit,
    out_pool_weight,
    out_attn_weight,
):
    lane = np.arange(128)
    freq = (rope_base ** (-(lane % 16) / 16.0)).astype(np.float32)[None]
    mixed, log_weight = whole_layer(
        tokens,
        (query_weight, key_weight, value_weight, pool_in_weight, out_pool_weight.T, out_attn_weight.T),
        norm_gain[None],
        pool_mix_weight,
        jnp.asarray(freq),
        sink_logit,
    )
    return (mixed, log_weight)


def solution(mesh):
    finer = Mesh(mesh.devices.reshape(8, 8, 2, mesh.shape["tp"]), ("sp_0", "sp_1", "sp_2", "tp"))
    placed = (
        P(SP, "tp"),
        P(),
        P(SP, "tp"),
        P(SP, "tp"),
        P(SP, "tp"),
        P(SP, "tp"),
        P("tp", None, None),
        P("tp"),
        P("tp", SP),
        P("tp", SP),
    )
    return jax.shard_map(
        local, mesh=finer, in_specs=placed, out_specs=(P(SP, "tp"), P("tp", SP)), check_vma=False
    )
```

```python
import jax
import jax.numpy as jnp
import numpy as np
from jax import lax
from jax.sharding import Mesh
from jax.experimental import pallas as pl
from jax.experimental.pallas import tpu as pltpu
from jax.sharding import PartitionSpec as P

HD = 64
GRID_W = 64
SP = ("sp_0", "sp_1", "sp_2")


norm_eps = 1e-06
rope_base = 10000.0
neg_fill = -1e30


MESH = pl.DeviceIdType.MESH
AX_Z, AX_Y, AX_C, AX_X = "sp_0", "sp_1", "sp_2", "tp"
BLOCK = 128
EDGE = 16


def remote(src, dst, send_sem, recv_sem, device):
    return pltpu.make_async_remote_copy(
        src_ref=src,
        dst_ref=dst,
        send_sem=send_sem,
        recv_sem=recv_sem,
        device_id=device,
        device_id_type=MESH,
    )


def wait_bytes(ref, sem):
    pltpu.make_async_copy(ref, ref, sem).wait()


class Torus:
    def __init__(self, buf, first, size, sems):
        self.buf, self.first, self.size = buf, first, size
        self.p1_send, self.p1_recv, self.p2_send, self.p2_recv, self.d_send, self.d_recv = sems
        self.z, self.y, self.c = lax.axis_index(AX_Z), lax.axis_index(AX_Y), lax.axis_index(AX_C)
        by_y = first == AX_Y
        self.n1, self.n2 = (buf.shape[1], buf.shape[0]) if by_y else (buf.shape[0], buf.shape[1])
        self.a, self.b = (self.y, self.z) if by_y else (self.z, self.y)
        self.second = AX_Z if by_y else AX_Y
        self.groups = self.n1 // size

    def chunk(self, b, start, size):
        if self.first == AX_Y:
            return self.buf.at[b, pl.ds(start, size), self.c]
        return self.buf.at[pl.ds(start, size), b, self.c]

    def group_id(self, k):
        return lax.rem(lax.div(self.a, self.size) + k, self.groups)

    def hops(self, way, k):
        half = self.n2 // 2
        return half if (way == 0) == (k < self.groups // 2) else half - 1

    def phase1_start(self):
        own = self.buf.at[self.z, self.y, self.c]
        order = sorted(range(1, self.n1), key=lambda d: min(d, self.n1 - d))
        for d in order:
            remote(
                own, own, self.p1_send, self.p1_recv.at[self.group_id(0)],
                {self.first: lax.rem(self.a + d, self.n1)},
            ).start()

    def to_partner(self, ref):
        remote(ref, ref, self.d_send, self.d_recv, {AX_C: 1 - self.c}).start()

    def phase1_group(self, k):
        count = self.size - 1 if k == 0 else self.size
        wait_bytes(self.chunk(self.b, 0, count), self.p1_recv.at[self.group_id(k)])
        for way in range(2):
            self.relay(way, k, 1).start()

    def block(self, way, k, back):
        step = 1 if way == 0 else self.n2 - 1
        origin = lax.rem(self.b + back * (self.n2 - step), self.n2)
        return self.chunk(origin, self.group_id(k) * self.size, self.size)

    def relay(self, way, k, hop):
        step = 1 if way == 0 else self.n2 - 1
        ref = self.block(way, k, hop - 1)
        return remote(
            ref, ref, self.p2_send.at[way, k, hop - 1], self.p2_recv.at[way, k, hop - 1],
            {self.second: lax.rem(self.b + step, self.n2)},
        )

    def level(self, hop, k, way):
        last = self.hops(way, k)
        if hop > last + 1:
            return
        ref = self.block(way, k, hop - 1)
        wait_bytes(ref, self.p2_recv.at[way, k, hop - 2])
        if hop <= last:
            self.relay(way, k, hop).start()

    def share(self, back):
        for way in range(1 if 2 * back in (0, self.n2) else 2):
            step = 1 if way == 0 else self.n2 - 1
            origin = lax.rem(self.b + back * (self.n2 - step), self.n2)
            self.to_partner(self.chunk(origin, 0, self.n1))

    def arrived(self):
        wait_bytes(self.buf.at[:, :, 1 - self.c], self.d_recv)

    def drain(self):
        wait_bytes(self.buf.at[:, :, self.c], self.d_send)
        wait_bytes(self.chunk(self.b, 0, self.n1 - 1), self.p1_send)
        for k in range(self.groups):
            for way in range(2):
                for hop in range(1, self.hops(way, k) + 1):
                    self.relay(way, k, hop).wait_send()


def torus_sems(n1, n2, size):
    dma = pltpu.SemaphoreType.DMA
    groups, hops = n1 // size, n2 // 2
    return [
        dma(()), dma((groups,)), dma((2, groups, hops)), dma((2, groups, hops)), dma(()), dma(()),
    ]


class Ring:
    def __init__(self, buf, sems):
        self.buf = buf
        self.send, self.recv = sems
        self.n, self.x = buf.shape[0], lax.axis_index(AX_X)
        self.half = buf.shape[1] // 2

    def part(self, x, which):
        return self.buf.at[x, which * self.half : (which + 1) * self.half]

    def copy(self, way, index, x, which):
        step = 1 if way == 0 else self.n - 1
        ref = self.part(x, which)
        return remote(
            ref, ref, self.send.at[way, index], self.recv.at[way, index],
            {AX_X: lax.rem(self.x + step, self.n)},
        )

    def start(self):
        for index in range(2):
            for way in range(2):
                self.copy(way, index, self.x, index if way == 0 else 1 - index).start()

    def forward(self):
        for way in range(2):
            step = 1 if way == 0 else self.n - 1
            behind = lax.rem(self.x + self.n - step, self.n)
            wait_bytes(self.part(behind, way), self.recv.at[way, 0])
            self.copy(way, 2, behind, way).start()

    def arrived(self):
        for way in range(2):
            step = 1 if way == 0 else self.n - 1
            behind = lax.rem(self.x + self.n - step, self.n)
            across = lax.rem(self.x + 2, self.n)
            wait_bytes(self.part(behind, 1 - way), self.recv.at[way, 1])
            wait_bytes(self.part(across, way), self.recv.at[way, 2])

    def drain(self):
        for way in range(2):
            for index in range(3):
                self.copy(way, index, self.x, 0).wait_send()


def sequence_neighbour(step):
    nz, ny, nc = (lax.axis_size(a) for a in (AX_Z, AX_Y, AX_C))
    place = (lax.axis_index(AX_Z) * ny + lax.axis_index(AX_Y)) * nc + lax.axis_index(AX_C)
    place = lax.rem(place + step + nz * ny * nc, nz * ny * nc)
    chip = lax.div(place, nc)
    return {AX_Z: lax.div(chip, ny), AX_Y: lax.rem(chip, ny), AX_C: lax.rem(place, nc)}


def greet_all():
    nz, ny, nx = (lax.axis_size(a) for a in (AX_Z, AX_Y, AX_X))
    z, y, c, x = (lax.axis_index(a) for a in (AX_Z, AX_Y, AX_C, AX_X))
    peers = [sequence_neighbour(1), sequence_neighbour(-1), {AX_C: 1 - c}]
    peers += [{AX_X: lax.rem(x + d, nx)} for d in (1, nx - 1)]
    peers += [{AX_Y: lax.rem(y + d, ny)} for d in range(1, ny)]
    peers += [{AX_Z: lax.rem(z + d, nz)} for d in range(1, nz)]
    barrier = pltpu.get_barrier_semaphore()
    for peer in peers:
        pl.semaphore_signal(barrier, inc=1, device_id=peer, device_id_type=MESH)
    pl.semaphore_wait(barrier, len(peers))


def turned(values, cosine, sine):
    lane = lax.broadcasted_iota(jnp.int32, values.shape, 1)
    ahead = pltpu.roll(values, 112, 1)
    behind = pltpu.roll(values, 16, 1)
    return values * cosine + jnp.where(lax.rem(lane, 32) < 16, ahead, behind) * sine


def rounded(values):
    return values.astype(jnp.bfloat16).astype(jnp.float32)


def fill_tables(place, freq_ref, cos_buf, sin_buf):
    row = (lax.broadcasted_iota(jnp.int32, (8, 128), 0) + place * 8).astype(jnp.float32)
    row_cos, row_sin = jnp.cos(row * freq_ref[0:1]), jnp.sin(row * freq_ref[0:1])
    col = lax.broadcasted_iota(jnp.int32, (GRID_W, 128), 0).astype(jnp.float32)
    col_cos, col_sin = jnp.cos(col * freq_ref[0:1]), jnp.sin(col * freq_ref[0:1])
    lane = lax.broadcasted_iota(jnp.int32, (GRID_W, 128), 1)
    by_row = lax.rem(lane, 64) < 32
    sign = jnp.where(lax.rem(lane, 32) < 16, -1.0, 1.0)
    for r in range(8):
        rows = slice(r * GRID_W, (r + 1) * GRID_W)
        cos_buf[rows] = jnp.where(by_row, row_cos[r : r + 1], col_cos)
        sin_buf[rows] = jnp.where(by_row, row_sin[r : r + 1], col_sin) * sign


def rows_of(buf, start, size, columns):
    parts = buf[start // 256 : (start + size) // 256, :, :, :, columns]
    return parts.reshape(size, -1)


def normalise(t_buf, gain_ref, normed):
    def step(i, carry):
        rows = pl.ds(pl.multiple_of(i * BLOCK, BLOCK), BLOCK)
        parts = [t_buf[k, rows, :].astype(jnp.float32) for k in range(4)]
        total = sum(jnp.sum(p * p, axis=-1, keepdims=True) for p in parts)
        scale = lax.rsqrt(total / 2048.0 + norm_eps)
        for k in range(4):
            cols = slice(k * 512, (k + 1) * 512)
            normed[rows, cols] = (parts[k] * scale * gain_ref[0:1, cols]).astype(jnp.bfloat16)
        return carry

    lax.fori_loop(0, 4, step, 0)


def project_keys(normed, wb, cos_ref, sin_ref, kv_ext):
    both = jnp.dot(
        normed[...], rows_of(wb, 0, 2048, slice(0, 256)), preferred_element_type=jnp.float32
    )
    keys = turned(rounded(both[:, :128]), cos_ref[...], sin_ref[...])
    kv_ext[BLOCK : BLOCK + 512, 0:128] = keys.astype(jnp.bfloat16)
    kv_ext[BLOCK : BLOCK + 512, 128:256] = both[:, 128:].astype(jnp.bfloat16)


def project_pool(normed, wb, pool_ext):
    pool_ext[EDGE : EDGE + 512, :] = jnp.dot(
        normed[...], rows_of(wb, 0, 2048, slice(256, 512)), preferred_element_type=jnp.float32
    ).astype(jnp.bfloat16)


def project_queries(normed, wa, cos_ref, sin_ref, queries, h):
    cols = slice(h * 256, (h + 1) * 256)
    found = jnp.dot(normed[...], rows_of(wa, 0, 2048, cols), preferred_element_type=jnp.float32)
    for pair in range(2):
        values = turned(
            rounded(found[:, pair * 128 : (pair + 1) * 128]), cos_ref[...], sin_ref[...]
        ) * (HD**-0.5)
        lane = lax.broadcasted_iota(jnp.int32, values.shape, 1)
        mine = (lane < 64) if h == 0 else (lane >= 64)
        for odd in range(2):
            placed = values if odd == h else pltpu.roll(values, 64, 1)
            placed = jnp.where(mine, placed, 0.0).astype(jnp.bfloat16)
            g = pair * 2 + odd
            for b in range(4):
                queries[h, b, g * BLOCK : (g + 1) * BLOCK, :] = placed[b * BLOCK : (b + 1) * BLOCK]


def attend(b, h, place, places, kv_ext, queries, sink_ref, features, log_ref):
    start = pl.multiple_of(b * BLOCK, BLOCK)
    keys = kv_ext[pl.ds(start, 3 * BLOCK), 0:128]
    scores = lax.dot_general(
        keys, queries[h, b], (((1,), (1,)), ((), ())), preferred_element_type=jnp.float32
    )
    shape = (BLOCK, 4 * BLOCK)
    key = lax.broadcasted_iota(jnp.int32, shape, 0)
    query = lax.rem(lax.broadcasted_iota(jnp.int32, shape, 1), BLOCK)
    first = jnp.where((place == 0) & (b == 0), BLOCK, 0)
    last = jnp.where((place == places - 1) & (b == 3), -1, BLOCK)
    before = jnp.where(key >= jnp.maximum(query, first), scores[:BLOCK], neg_fill)
    here = scores[BLOCK : 2 * BLOCK]
    after = jnp.where(key <= jnp.minimum(query, last), scores[2 * BLOCK :], neg_fill)
    sink = jnp.concatenate([jnp.full((1, BLOCK), sink_ref[4 * h + g], jnp.float32) for g in range(4)], 1)
    top = jnp.max(jnp.maximum(jnp.maximum(before, here), after), axis=0, keepdims=True)
    top = jnp.maximum(top, sink)
    exps = [jnp.exp(part - top) for part in (before, here, after)]
    total = jnp.sum(exps[0] + exps[1] + exps[2], axis=0, keepdims=True) + jnp.exp(sink - top)
    logs = top + jnp.log(total)
    weights = jnp.concatenate([e.astype(jnp.bfloat16) for e in exps], axis=0)
    values = kv_ext[pl.ds(start, 3 * BLOCK), 128:256]
    summed = lax.dot_general(
        values, weights, (((0,), (0,)), ((), ())), preferred_element_type=jnp.float32
    )
    mine = summed[h * 64 : (h + 1) * 64] / total
    for g in range(4):
        log_ref[4 * h + g : 4 * h + g + 1, pl.ds(start, BLOCK)] = logs[
            :, g * BLOCK : (g + 1) * BLOCK
        ]
    for pair in range(2):
        two = jnp.concatenate(
            [mine[:, (2 * pair + e) * BLOCK : (2 * pair + e + 1) * BLOCK] for e in range(2)], axis=0
        )
        at = 256 + h * 256 + pair * 128
        features[pl.ds(start, BLOCK), at : at + 128] = two.T.astype(jnp.bfloat16)


def pool(b, place, places, reach, pool_ext, mix_ref, features):
    start = pl.multiple_of(b * BLOCK, BLOCK)
    size = BLOCK + 2 * EDGE
    base = place * 512 + b * BLOCK
    row = lax.broadcasted_iota(jnp.int32, (BLOCK, size), 0)
    col = lax.broadcasted_iota(jnp.int32, (BLOCK, size), 1) - EDGE
    inside = (col >= row - reach) & (col < row + reach)
    inside = inside & (col >= -base) & (col < places * 512 - base)
    band = jnp.where(inside, 1.0, 0.0)
    counted = jnp.sum(band, axis=-1, keepdims=True)
    ext = pool_ext[pl.ds(start, size), :]
    summed = jnp.dot(band.astype(jnp.bfloat16), ext, preferred_element_type=jnp.float32)
    own = ext[EDGE : EDGE + BLOCK].astype(jnp.float32)
    pooled = (summed / counted - own).astype(jnp.bfloat16)
    features[pl.ds(start, BLOCK), 0:256] = jnp.dot(
        pooled, mix_ref[0], preferred_element_type=jnp.float32
    ).astype(jnp.bfloat16)


def partial_term(b, j, features, oa, ob):
    rows = pl.ds(pl.multiple_of(b * BLOCK, BLOCK), BLOCK)
    dims = (((1,), (1,)), ((), ()))
    low = oa[pl.ds(2 * j, 2)].reshape(512, 384)
    high = ob[pl.ds(2 * j, 2)].reshape(512, 384)
    return lax.dot_general(
        features[rows, 0:384], low, dims, preferred_element_type=jnp.float32
    ) + lax.dot_general(features[rows, 384:768], high, dims, preferred_element_type=jnp.float32)


class Scatter:
    def __init__(self, refs, sems):
        self.far, self.near, self.far_in, self.near_in, self.kept = refs
        self.far_send, self.far_recv, self.near_send, self.near_recv = sems
        self.n, self.x = lax.axis_size(AX_X), lax.axis_index(AX_X)
        self.half = BLOCK // 2

    def target(self, way):
        return lax.rem(self.x + (1 if way == 0 else self.n - 1), self.n)

    def far_copy(self, b, way):
        rows = slice(way * self.half, (way + 1) * self.half)
        return remote(
            self.far.at[b, rows], self.far_in.at[b, way],
            self.far_send.at[b, way], self.far_recv.at[b, way], {AX_X: self.target(way)},
        )

    def near_copy(self, b, way, added):
        which = way if added else 1 - way
        rows = slice(which * self.half, (which + 1) * self.half)
        index = 1 if added else 0
        return remote(
            self.near.at[b, way, rows], self.near_in.at[b, way, rows],
            self.near_send.at[b, way, index], self.near_recv.at[b, way, index],
            {AX_X: self.target(way)},
        )

    def compute(self, b, features, oa, ob):
        across = lax.rem(self.x + 2, self.n)
        self.far[b] = partial_term(b, across, features, oa, ob).astype(jnp.bfloat16)
        for way in range(2):
            self.far_copy(b, way).start()
        for way in range(2):
            self.near[b, way] = partial_term(b, self.target(way), features, oa, ob).astype(jnp.bfloat16)
            self.near_copy(b, way, False).start()
        self.kept[b] = partial_term(b, self.x, features, oa, ob).astype(jnp.bfloat16)

    def add(self, b):
        for way in range(2):
            rows = slice(way * self.half, (way + 1) * self.half)
            self.far_copy(b, way).wait_recv()
            both = self.near[b, way, rows].astype(jnp.float32) + self.far_in[b, way].astype(jnp.float32)
            self.near[b, way, rows] = both.astype(jnp.bfloat16)
            self.near_copy(b, way, True).start()

    def finish(self, b, out_ref):
        for way in range(2):
            for added in (False, True):
                self.near_copy(b, way, added).wait_recv()
        total = self.kept[b].astype(jnp.float32)
        for way in range(2):
            total = total + self.near_in[b, way].astype(jnp.float32)
        out_ref[pl.ds(pl.multiple_of(b * BLOCK, BLOCK), BLOCK), :] = total.astype(jnp.bfloat16)

    def drain(self, b):
        for way in range(2):
            self.far_copy(b, way).wait_send()
            for added in (False, True):
                self.near_copy(b, way, added).wait_send()


def layer_kernel(
    tok_ref, q_ref, k_ref, v_ref, p_ref, op_ref, oq_ref,
    gain_hbm, mix_hbm, freq_ref, sink_ref,
    out_ref, log_ref,
    t_buf, wa, wb, oa, ob, gain_ref, mix_ref, cos_ref, sin_ref, normed, queries, kv_ext, pool_ext, features,
    far, near, far_in, near_in, kept,
    load_sem, ring_send, ring_recv, halo_send, halo_recv, far_send, far_recv, near_send, near_recv,
    *torus,
):
    z, y, c, x = (lax.axis_index(a) for a in (AX_Z, AX_Y, AX_C, AX_X))
    nz, ny, nc = (lax.axis_size(a) for a in (AX_Z, AX_Y, AX_C))
    place, places = (z * ny + y) * nc + c, nz * ny * nc
    ring = Ring(t_buf, (ring_send, ring_recv))
    ins = [Torus(wa, AX_Y, 4, torus[0:6]), Torus(wb, AX_Z, 4, torus[6:12])]
    outs = [Torus(oa, AX_Y, 4, torus[12:18]), Torus(ob, AX_Z, 4, torus[18:24])]
    loads = [
        pltpu.make_async_copy(tok_ref, t_buf.at[x], load_sem.at[0]),
        pltpu.make_async_copy(q_ref, wa.at[z, y, c], load_sem.at[1]),
        pltpu.make_async_copy(k_ref, wb.at[z, y, c, :, 0:128], load_sem.at[2]),
        pltpu.make_async_copy(v_ref, wb.at[z, y, c, :, 128:256], load_sem.at[3]),
        pltpu.make_async_copy(p_ref, wb.at[z, y, c, :, 256:512], load_sem.at[4]),
        pltpu.make_async_copy(op_ref, oa.at[z, y, c, :, 0:256], load_sem.at[5]),
        pltpu.make_async_copy(oq_ref.at[:, 0:128], oa.at[z, y, c, :, 256:384], load_sem.at[6]),
        pltpu.make_async_copy(oq_ref.at[:, 128:512], ob.at[z, y, c], load_sem.at[7]),
    ]
    later = [
        pltpu.make_async_copy(gain_hbm, gain_ref, load_sem.at[8]),
        pltpu.make_async_copy(mix_hbm, mix_ref, load_sem.at[9]),
    ]
    for load in loads + later:
        load.start()
    greet_all()
    for load in loads:
        load.wait()
    for t in ins:
        t.phase1_start()
    ring.start()
    for load in later:
        load.wait()
    fill_tables(place, freq_ref, cos_ref, sin_ref)

    def first(group):
        for k in range(group[0].groups):
            for t in group:
                t.phase1_group(k)
        for t in group:
            t.share(0)

    def levels(group, hop):
        for k in range(group[0].groups):
            for way in range(2):
                for t in group:
                    t.level(hop, k, way)
        for t in group:
            t.share(hop - 1)


    def halo_copies(way):
        low = 512 if way == 0 else BLOCK
        high = 0 if way == 0 else BLOCK + 512
        plow = 512 if way == 0 else EDGE
        phigh = 0 if way == 0 else EDGE + 512
        device = sequence_neighbour(1 if way == 0 else -1)
        return [
            remote(
                kv_ext.at[low : low + BLOCK], kv_ext.at[high : high + BLOCK],
                halo_send.at[way, 0], halo_recv.at[way, 0], device,
            ),
            remote(
                pool_ext.at[plow : plow + EDGE], pool_ext.at[phigh : phigh + EDGE],
                halo_send.at[way, 1], halo_recv.at[way, 1], device,
            ),
        ]

    reach = lax.shift_left(jnp.int32(1), x)
    scatter = Scatter(
        (far, near, far_in, near_in, kept), (far_send, far_recv, near_send, near_recv)
    )

    def block(i, carry):
        b = lax.rem(i + 1, 4)
        for h in range(2):
            attend(b, h, place, places, kv_ext, queries, sink_ref, features, log_ref)
        pool(b, place, places, reach, pool_ext, mix_ref, features)
        return carry

    def send(i, carry):
        b = lax.rem(i + 1, 4)
        scatter.compute(b, features, oa, ob)

        @pl.when(i > 0)
        def _():
            scatter.add(i)

        return carry

    def both(i, carry):
        block(i, carry)
        return send(i, carry)

    for t in outs:
        t.phase1_start()
    first(ins)
    levels(ins, 2)
    ring.forward()
    first(outs)
    levels(ins, 3)
    levels(outs, 2)
    levels(ins, 4)
    levels(outs, 3)
    ring.arrived()
    normalise(t_buf, gain_ref, normed)
    levels(ins, 5)
    for t in ins:
        t.arrived()
    project_keys(normed, wb, cos_ref, sin_ref, kv_ext)
    project_pool(normed, wb, pool_ext)
    for way in range(2):
        for copy in halo_copies(way):
            copy.start()
    project_queries(normed, wa, cos_ref, sin_ref, queries, 0)
    levels(outs, 4)
    project_queries(normed, wa, cos_ref, sin_ref, queries, 1)
    block(0, 0)
    levels(outs, 5)
    for t in outs:
        t.arrived()
    send(0, 0)
    lax.fori_loop(1, 2, both, 0)
    for way in range(2):
        for copy in halo_copies(way):
            copy.wait_recv()
    lax.fori_loop(2, 4, both, 0)
    scatter.add(0)

    def close(i, carry):
        b = lax.rem(i + 1, 4)
        scatter.finish(b, out_ref)
        scatter.drain(b)
        return carry

    lax.fori_loop(0, 4, close, 0)
    for t in ins + outs:
        t.drain()
    ring.drain()
    for way in range(2):
        for copy in halo_copies(way):
            copy.wait_send()


def whole_layer(tokens, weights, gain, mix, freq, sink):
    nz, ny, nc, nx = (lax.axis_size(a) for a in (AX_Z, AX_Y, AX_C, AX_X))
    rows, width = tokens.shape
    bf = jnp.bfloat16
    dma = pltpu.SemaphoreType.DMA
    vmem = pltpu.VMEM
    blocks = rows // BLOCK
    near_data = pl.BlockSpec(memory_space=pltpu.VMEM)
    return pl.pallas_call(
        layer_kernel,
        out_shape=[
            vmem((rows, width), bf),
            vmem((8, rows), jnp.float32),
        ],
        in_specs=[pl.BlockSpec(memory_space=pltpu.HBM)] * 9 + [near_data]
        + [pl.BlockSpec(memory_space=pltpu.SMEM)],
        out_specs=[near_data] * 2,
        scratch_shapes=[
            vmem((nx, rows, width), bf),
            vmem((nz, ny, nc, 16, 512), bf),
            vmem((nz, ny, nc, 16, 512), bf),
            vmem((nz, ny, nc, 16, 384), bf),
            vmem((nz, ny, nc, 16, 384), bf),
            vmem((1, nx * width), jnp.float32),
            vmem((1, 256, 256), bf),
            vmem((rows, 128), jnp.float32),
            vmem((rows, 128), jnp.float32),
            vmem((rows, nx * width), bf),
            vmem((2, blocks, 4 * BLOCK, 128), bf),
            vmem((rows + 2 * BLOCK, 256), bf),
            vmem((rows + 2 * EDGE, 256), bf),
            vmem((rows, 768), bf),
            vmem((blocks, BLOCK, 512), bf),
            vmem((blocks, 2, BLOCK, 512), bf),
            vmem((blocks, 2, BLOCK // 2, 512), bf),
            vmem((blocks, 2, BLOCK, 512), bf),
            vmem((blocks, BLOCK, 512), bf),
            dma((10,)), dma((2, 3)), dma((2, 3)), dma((2, 2)), dma((2, 2)),
            dma((blocks, 2)), dma((blocks, 2)), dma((blocks, 2, 2)), dma((blocks, 2, 2)),
        ]
        + torus_sems(ny, nz, 4) + torus_sems(nz, ny, 4) + torus_sems(ny, nz, 4) + torus_sems(nz, ny, 4),
        compiler_params=pltpu.CompilerParams(
            collective_id=0, has_side_effects=True, vmem_limit_bytes=56 * 1024 * 1024
        ),
    )(tokens, *weights, gain, mix, freq, sink)


def local(
    tokens,
    norm_gain,
    query_weight,
    key_weight,
    value_weight,
    pool_in_weight,
    pool_mix_weight,
    sink_logit,
    out_pool_weight,
    out_attn_weight,
):
    lane = np.arange(128)
    freq = (rope_base ** (-(lane % 16) / 16.0)).astype(np.float32)[None]
    mixed, log_weight = whole_layer(
        tokens,
        (query_weight, key_weight, value_weight, pool_in_weight, out_pool_weight.T, out_attn_weight.T),
        norm_gain[None],
        pool_mix_weight,
        jnp.asarray(freq),
        sink_logit,
    )
    return (mixed, log_weight)


def solution(mesh):
    finer = Mesh(mesh.devices.reshape(8, 8, 2, mesh.shape["tp"]), ("sp_0", "sp_1", "sp_2", "tp"))
    placed = (
        P(SP, "tp"),
        P(),
        P(SP, "tp"),
        P(SP, "tp"),
        P(SP, "tp"),
        P(SP, "tp"),
        P("tp", None, None),
        P("tp"),
        P("tp", SP),
        P("tp", SP),
    )
    return jax.shard_map(
        local, mesh=finer, in_specs=placed, out_specs=(P(SP, "tp"), P("tp", SP)), check_vma=False
    )
```

```python
import jax
import jax.numpy as jnp
import numpy as np
from jax import lax
from jax.sharding import Mesh
from jax.experimental import pallas as pl
from jax.experimental.pallas import tpu as pltpu
from jax.sharding import PartitionSpec as P

HD = 64
GRID_W = 64
SP = ("sp_0", "sp_1", "sp_2")


norm_eps = 1e-06
rope_base = 10000.0
neg_fill = -1e30


MESH = pl.DeviceIdType.MESH
AX_Z, AX_Y, AX_C, AX_X = "sp_0", "sp_1", "sp_2", "tp"
BLOCK = 128
EDGE = 16


def remote(src, dst, send_sem, recv_sem, device):
    return pltpu.make_async_remote_copy(
        src_ref=src,
        dst_ref=dst,
        send_sem=send_sem,
        recv_sem=recv_sem,
        device_id=device,
        device_id_type=MESH,
    )


def wait_bytes(ref, sem):
    pltpu.make_async_copy(ref, ref, sem).wait()


class Torus:
    def __init__(self, buf, first, size, sems):
        self.buf, self.first, self.size = buf, first, size
        self.p1_send, self.p1_recv, self.p2_send, self.p2_recv, self.d_send, self.d_recv = sems
        self.z, self.y, self.c = lax.axis_index(AX_Z), lax.axis_index(AX_Y), lax.axis_index(AX_C)
        by_y = first == AX_Y
        self.n1, self.n2 = (buf.shape[1], buf.shape[0]) if by_y else (buf.shape[0], buf.shape[1])
        self.a, self.b = (self.y, self.z) if by_y else (self.z, self.y)
        self.second = AX_Z if by_y else AX_Y
        self.groups = self.n1 // size

    def chunk(self, b, start, size):
        if self.first == AX_Y:
            return self.buf.at[b, pl.ds(start, size), self.c]
        return self.buf.at[pl.ds(start, size), b, self.c]

    def group_id(self, k):
        return lax.rem(lax.div(self.a, self.size) + k, self.groups)

    def hops(self, way, k):
        half = self.n2 // 2
        return half if (way == 0) == (k < self.groups // 2) else half - 1

    def phase1_start(self):
        own = self.buf.at[self.z, self.y, self.c]
        order = sorted(range(1, self.n1), key=lambda d: min(d, self.n1 - d))
        for d in order:
            remote(
                own, own, self.p1_send, self.p1_recv.at[self.group_id(0)],
                {self.first: lax.rem(self.a + d, self.n1)},
            ).start()

    def to_partner(self, ref):
        remote(ref, ref, self.d_send, self.d_recv, {AX_C: 1 - self.c}).start()

    def phase1_group(self, k):
        count = self.size - 1 if k == 0 else self.size
        wait_bytes(self.chunk(self.b, 0, count), self.p1_recv.at[self.group_id(k)])
        for way in range(2):
            self.relay(way, k, 1).start()

    def block(self, way, k, back):
        step = 1 if way == 0 else self.n2 - 1
        origin = lax.rem(self.b + back * (self.n2 - step), self.n2)
        return self.chunk(origin, self.group_id(k) * self.size, self.size)

    def relay(self, way, k, hop):
        step = 1 if way == 0 else self.n2 - 1
        ref = self.block(way, k, hop - 1)
        return remote(
            ref, ref, self.p2_send.at[way, k, hop - 1], self.p2_recv.at[way, k, hop - 1],
            {self.second: lax.rem(self.b + step, self.n2)},
        )

    def level(self, hop, k, way):
        last = self.hops(way, k)
        if hop > last + 1:
            return
        ref = self.block(way, k, hop - 1)
        wait_bytes(ref, self.p2_recv.at[way, k, hop - 2])
        if hop <= last:
            self.relay(way, k, hop).start()

    def share(self, back):
        for way in range(1 if 2 * back in (0, self.n2) else 2):
            step = 1 if way == 0 else self.n2 - 1
            origin = lax.rem(self.b + back * (self.n2 - step), self.n2)
            self.to_partner(self.chunk(origin, 0, self.n1))

    def arrived(self):
        wait_bytes(self.buf.at[:, :, 1 - self.c], self.d_recv)

    def drain(self):
        wait_bytes(self.buf.at[:, :, self.c], self.d_send)
        wait_bytes(self.chunk(self.b, 0, self.n1 - 1), self.p1_send)
        for k in range(self.groups):
            for way in range(2):
                for hop in range(1, self.hops(way, k) + 1):
                    self.relay(way, k, hop).wait_send()


def torus_sems(n1, n2, size):
    dma = pltpu.SemaphoreType.DMA
    groups, hops = n1 // size, n2 // 2
    return [
        dma(()), dma((groups,)), dma((2, groups, hops)), dma((2, groups, hops)), dma(()), dma(()),
    ]


class Ring:
    def __init__(self, buf, sems):
        self.buf = buf
        self.send, self.recv = sems
        self.n, self.x = buf.shape[0], lax.axis_index(AX_X)
        self.half = buf.shape[1] // 2

    def part(self, x, which):
        return self.buf.at[x, which * self.half : (which + 1) * self.half]

    def copy(self, way, index, x, which):
        step = 1 if way == 0 else self.n - 1
        ref = self.part(x, which)
        return remote(
            ref, ref, self.send.at[way, index], self.recv.at[way, index],
            {AX_X: lax.rem(self.x + step, self.n)},
        )

    def start(self):
        for index in range(2):
            for way in range(2):
                self.copy(way, index, self.x, index if way == 0 else 1 - index).start()

    def forward(self):
        for way in range(2):
            step = 1 if way == 0 else self.n - 1
            behind = lax.rem(self.x + self.n - step, self.n)
            wait_bytes(self.part(behind, way), self.recv.at[way, 0])
            self.copy(way, 2, behind, way).start()

    def arrived(self):
        for way in range(2):
            step = 1 if way == 0 else self.n - 1
            behind = lax.rem(self.x + self.n - step, self.n)
            across = lax.rem(self.x + 2, self.n)
            wait_bytes(self.part(behind, 1 - way), self.recv.at[way, 1])
            wait_bytes(self.part(across, way), self.recv.at[way, 2])

    def drain(self):
        for way in range(2):
            for index in range(3):
                self.copy(way, index, self.x, 0).wait_send()


def sequence_neighbour(step):
    nz, ny, nc = (lax.axis_size(a) for a in (AX_Z, AX_Y, AX_C))
    place = (lax.axis_index(AX_Z) * ny + lax.axis_index(AX_Y)) * nc + lax.axis_index(AX_C)
    place = lax.rem(place + step + nz * ny * nc, nz * ny * nc)
    chip = lax.div(place, nc)
    return {AX_Z: lax.div(chip, ny), AX_Y: lax.rem(chip, ny), AX_C: lax.rem(place, nc)}


def greet_all():
    nz, ny, nx = (lax.axis_size(a) for a in (AX_Z, AX_Y, AX_X))
    z, y, c, x = (lax.axis_index(a) for a in (AX_Z, AX_Y, AX_C, AX_X))
    peers = [sequence_neighbour(1), sequence_neighbour(-1), {AX_C: 1 - c}]
    peers += [{AX_X: lax.rem(x + d, nx)} for d in (1, nx - 1)]
    peers += [{AX_Y: lax.rem(y + d, ny)} for d in range(1, ny)]
    peers += [{AX_Z: lax.rem(z + d, nz)} for d in range(1, nz)]
    barrier = pltpu.get_barrier_semaphore()
    for peer in peers:
        pl.semaphore_signal(barrier, inc=1, device_id=peer, device_id_type=MESH)
    pl.semaphore_wait(barrier, len(peers))


def turned(values, cosine, sine):
    lane = lax.broadcasted_iota(jnp.int32, values.shape, 1)
    ahead = pltpu.roll(values, 112, 1)
    behind = pltpu.roll(values, 16, 1)
    return values * cosine + jnp.where(lax.rem(lane, 32) < 16, ahead, behind) * sine


def rounded(values):
    return values.astype(jnp.bfloat16).astype(jnp.float32)


def fill_tables(place, freq_ref, cos_buf, sin_buf):
    row = (lax.broadcasted_iota(jnp.int32, (8, 128), 0) + place * 8).astype(jnp.float32)
    row_cos, row_sin = jnp.cos(row * freq_ref[0:1]), jnp.sin(row * freq_ref[0:1])
    col = lax.broadcasted_iota(jnp.int32, (GRID_W, 128), 0).astype(jnp.float32)
    col_cos, col_sin = jnp.cos(col * freq_ref[0:1]), jnp.sin(col * freq_ref[0:1])
    lane = lax.broadcasted_iota(jnp.int32, (GRID_W, 128), 1)
    by_row = lax.rem(lane, 64) < 32
    sign = jnp.where(lax.rem(lane, 32) < 16, -1.0, 1.0)
    for r in range(8):
        rows = slice(r * GRID_W, (r + 1) * GRID_W)
        cos_buf[rows] = jnp.where(by_row, row_cos[r : r + 1], col_cos)
        sin_buf[rows] = jnp.where(by_row, row_sin[r : r + 1], col_sin) * sign


def rows_of(buf, start, size, columns):
    parts = buf[start // 256 : (start + size) // 256, :, :, :, columns]
    return parts.reshape(size, -1)


def normalise(t_buf, gain_ref, normed):
    def step(i, carry):
        rows = pl.ds(pl.multiple_of(i * BLOCK, BLOCK), BLOCK)
        parts = [t_buf[k, rows, :].astype(jnp.float32) for k in range(4)]
        total = sum(jnp.sum(p * p, axis=-1, keepdims=True) for p in parts)
        scale = lax.rsqrt(total / 2048.0 + norm_eps)
        for k in range(4):
            cols = slice(k * 512, (k + 1) * 512)
            normed[rows, cols] = (parts[k] * scale * gain_ref[0:1, cols]).astype(jnp.bfloat16)
        return carry

    lax.fori_loop(0, 4, step, 0)


def project_keys(normed, wb, cos_ref, sin_ref, kv_ext):
    both = jnp.dot(
        normed[...], rows_of(wb, 0, 2048, slice(0, 256)), preferred_element_type=jnp.float32
    )
    keys = turned(rounded(both[:, :128]), cos_ref[...], sin_ref[...])
    kv_ext[BLOCK : BLOCK + 512, 0:128] = keys.astype(jnp.bfloat16)
    kv_ext[BLOCK : BLOCK + 512, 128:256] = both[:, 128:].astype(jnp.bfloat16)


def project_pool(normed, wb, pool_ext):
    pool_ext[EDGE : EDGE + 512, :] = jnp.dot(
        normed[...], rows_of(wb, 0, 2048, slice(256, 512)), preferred_element_type=jnp.float32
    ).astype(jnp.bfloat16)


def project_queries(normed, wa, cos_ref, sin_ref, queries, h):
    cols = slice(h * 256, (h + 1) * 256)
    found = jnp.dot(normed[...], rows_of(wa, 0, 2048, cols), preferred_element_type=jnp.float32)
    for pair in range(2):
        values = turned(
            rounded(found[:, pair * 128 : (pair + 1) * 128]), cos_ref[...], sin_ref[...]
        ) * (HD**-0.5)
        lane = lax.broadcasted_iota(jnp.int32, values.shape, 1)
        mine = (lane < 64) if h == 0 else (lane >= 64)
        for odd in range(2):
            placed = values if odd == h else pltpu.roll(values, 64, 1)
            placed = jnp.where(mine, placed, 0.0).astype(jnp.bfloat16)
            g = pair * 2 + odd
            for b in range(4):
                queries[h, b, g * BLOCK : (g + 1) * BLOCK, :] = placed[b * BLOCK : (b + 1) * BLOCK]


def attend(b, h, place, places, kv_ext, queries, sink_ref, features, log_ref):
    start = pl.multiple_of(b * BLOCK, BLOCK)
    keys = kv_ext[pl.ds(start, 3 * BLOCK), 0:128]
    scores = lax.dot_general(
        keys, queries[h, b], (((1,), (1,)), ((), ())), preferred_element_type=jnp.float32
    )
    shape = (BLOCK, 4 * BLOCK)
    key = lax.broadcasted_iota(jnp.int32, shape, 0)
    query = lax.rem(lax.broadcasted_iota(jnp.int32, shape, 1), BLOCK)
    first = jnp.where((place == 0) & (b == 0), BLOCK, 0)
    last = jnp.where((place == places - 1) & (b == 3), -1, BLOCK)
    before = jnp.where(key >= jnp.maximum(query, first), scores[:BLOCK], neg_fill)
    here = scores[BLOCK : 2 * BLOCK]
    after = jnp.where(key <= jnp.minimum(query, last), scores[2 * BLOCK :], neg_fill)
    sink = jnp.concatenate([jnp.full((1, BLOCK), sink_ref[4 * h + g], jnp.float32) for g in range(4)], 1)
    top = jnp.max(jnp.maximum(jnp.maximum(before, here), after), axis=0, keepdims=True)
    top = jnp.maximum(top, sink)
    exps = [jnp.exp(part - top) for part in (before, here, after)]
    total = jnp.sum(exps[0] + exps[1] + exps[2], axis=0, keepdims=True) + jnp.exp(sink - top)
    logs = top + jnp.log(total)
    weights = jnp.concatenate([e.astype(jnp.bfloat16) for e in exps], axis=0)
    values = kv_ext[pl.ds(start, 3 * BLOCK), 128:256]
    summed = lax.dot_general(
        values, weights, (((0,), (0,)), ((), ())), preferred_element_type=jnp.float32
    )
    mine = summed[h * 64 : (h + 1) * 64] / total
    for g in range(4):
        log_ref[4 * h + g : 4 * h + g + 1, pl.ds(start, BLOCK)] = logs[
            :, g * BLOCK : (g + 1) * BLOCK
        ]
    for pair in range(2):
        two = jnp.concatenate(
            [mine[:, (2 * pair + e) * BLOCK : (2 * pair + e + 1) * BLOCK] for e in range(2)], axis=0
        )
        at = 256 + h * 256 + pair * 128
        features[pl.ds(start, BLOCK), at : at + 128] = two.T.astype(jnp.bfloat16)


def pool(b, place, places, reach, pool_ext, mix_ref, features):
    start = pl.multiple_of(b * BLOCK, BLOCK)
    size = BLOCK + 2 * EDGE
    base = place * 512 + b * BLOCK
    row = lax.broadcasted_iota(jnp.int32, (BLOCK, size), 0)
    col = lax.broadcasted_iota(jnp.int32, (BLOCK, size), 1) - EDGE
    inside = (col >= row - reach) & (col < row + reach)
    inside = inside & (col >= -base) & (col < places * 512 - base)
    band = jnp.where(inside, 1.0, 0.0)
    counted = jnp.sum(band, axis=-1, keepdims=True)
    ext = pool_ext[pl.ds(start, size), :]
    summed = jnp.dot(band.astype(jnp.bfloat16), ext, preferred_element_type=jnp.float32)
    own = ext[EDGE : EDGE + BLOCK].astype(jnp.float32)
    pooled = (summed / counted - own).astype(jnp.bfloat16)
    features[pl.ds(start, BLOCK), 0:256] = jnp.dot(
        pooled, mix_ref[0], preferred_element_type=jnp.float32
    ).astype(jnp.bfloat16)


def partial_term(b, j, features, oa, ob):
    rows = pl.ds(pl.multiple_of(b * BLOCK, BLOCK), BLOCK)
    dims = (((1,), (1,)), ((), ()))
    low = oa[pl.ds(2 * j, 2)].reshape(512, 384)
    high = ob[pl.ds(2 * j, 2)].reshape(512, 384)
    return lax.dot_general(
        features[rows, 0:384], low, dims, preferred_element_type=jnp.float32
    ) + lax.dot_general(features[rows, 384:768], high, dims, preferred_element_type=jnp.float32)


class Scatter:
    def __init__(self, refs, sems):
        self.far, self.near, self.far_in, self.near_in, self.kept = refs
        self.far_send, self.far_recv, self.near_send, self.near_recv = sems
        self.n, self.x = lax.axis_size(AX_X), lax.axis_index(AX_X)
        self.half = BLOCK // 2

    def target(self, way):
        return lax.rem(self.x + (1 if way == 0 else self.n - 1), self.n)

    def far_copy(self, b, way):
        rows = slice(way * self.half, (way + 1) * self.half)
        return remote(
            self.far.at[b, rows], self.far_in.at[b, way],
            self.far_send.at[b, way], self.far_recv.at[b, way], {AX_X: self.target(way)},
        )

    def near_copy(self, b, way, added):
        which = way if added else 1 - way
        rows = slice(which * self.half, (which + 1) * self.half)
        index = 1 if added else 0
        return remote(
            self.near.at[b, way, rows], self.near_in.at[b, way, rows],
            self.near_send.at[b, way, index], self.near_recv.at[b, way, index],
            {AX_X: self.target(way)},
        )

    def compute(self, b, features, oa, ob):
        across = lax.rem(self.x + 2, self.n)
        self.far[b] = partial_term(b, across, features, oa, ob).astype(jnp.bfloat16)
        for way in range(2):
            self.far_copy(b, way).start()
        for way in range(2):
            self.near[b, way] = partial_term(b, self.target(way), features, oa, ob).astype(jnp.bfloat16)
            self.near_copy(b, way, False).start()
        self.kept[b] = partial_term(b, self.x, features, oa, ob).astype(jnp.bfloat16)

    def add(self, b):
        for way in range(2):
            rows = slice(way * self.half, (way + 1) * self.half)
            self.far_copy(b, way).wait_recv()
            both = self.near[b, way, rows].astype(jnp.float32) + self.far_in[b, way].astype(jnp.float32)
            self.near[b, way, rows] = both.astype(jnp.bfloat16)
            self.near_copy(b, way, True).start()

    def finish(self, b, out_ref):
        for way in range(2):
            for added in (False, True):
                self.near_copy(b, way, added).wait_recv()
        total = self.kept[b].astype(jnp.float32)
        for way in range(2):
            total = total + self.near_in[b, way].astype(jnp.float32)
        out_ref[pl.ds(pl.multiple_of(b * BLOCK, BLOCK), BLOCK), :] = total.astype(jnp.bfloat16)

    def drain(self, b):
        for way in range(2):
            self.far_copy(b, way).wait_send()
            for added in (False, True):
                self.near_copy(b, way, added).wait_send()


def layer_kernel(
    tok_ref, q_ref, k_ref, v_ref, p_ref, op_ref, oq_ref,
    gain_hbm, mix_hbm, freq_ref, sink_ref,
    out_ref, log_ref,
    t_buf, wa, wb, oa, ob, gain_ref, mix_ref, cos_ref, sin_ref, normed, queries, kv_ext, pool_ext, features,
    far, near, far_in, near_in, kept,
    load_sem, ring_send, ring_recv, halo_send, halo_recv, far_send, far_recv, near_send, near_recv,
    *torus,
):
    z, y, c, x = (lax.axis_index(a) for a in (AX_Z, AX_Y, AX_C, AX_X))
    nz, ny, nc = (lax.axis_size(a) for a in (AX_Z, AX_Y, AX_C))
    place, places = (z * ny + y) * nc + c, nz * ny * nc
    ring = Ring(t_buf, (ring_send, ring_recv))
    ins = [Torus(wa, AX_Y, 4, torus[0:6]), Torus(wb, AX_Z, 4, torus[6:12])]
    outs = [Torus(oa, AX_Y, 8, torus[12:18]), Torus(ob, AX_Z, 8, torus[18:24])]
    loads = [
        pltpu.make_async_copy(tok_ref, t_buf.at[x], load_sem.at[0]),
        pltpu.make_async_copy(q_ref, wa.at[z, y, c], load_sem.at[1]),
        pltpu.make_async_copy(k_ref, wb.at[z, y, c, :, 0:128], load_sem.at[2]),
        pltpu.make_async_copy(v_ref, wb.at[z, y, c, :, 128:256], load_sem.at[3]),
        pltpu.make_async_copy(p_ref, wb.at[z, y, c, :, 256:512], load_sem.at[4]),
        pltpu.make_async_copy(op_ref, oa.at[z, y, c, :, 0:256], load_sem.at[5]),
        pltpu.make_async_copy(oq_ref.at[:, 0:128], oa.at[z, y, c, :, 256:384], load_sem.at[6]),
        pltpu.make_async_copy(oq_ref.at[:, 128:512], ob.at[z, y, c], load_sem.at[7]),
    ]
    later = [
        pltpu.make_async_copy(gain_hbm, gain_ref, load_sem.at[8]),
        pltpu.make_async_copy(mix_hbm, mix_ref, load_sem.at[9]),
    ]
    for load in loads + later:
        load.start()
    greet_all()
    for load in loads:
        load.wait()
    for t in ins:
        t.phase1_start()
    ring.start()
    for load in later:
        load.wait()
    fill_tables(place, freq_ref, cos_ref, sin_ref)

    def first(group):
        for k in range(group[0].groups):
            for t in group:
                t.phase1_group(k)
        for t in group:
            t.share(0)

    def levels(group, hop):
        for k in range(group[0].groups):
            for way in range(2):
                for t in group:
                    t.level(hop, k, way)
        for t in group:
            t.share(hop - 1)


    def halo_copies(way):
        low = 512 if way == 0 else BLOCK
        high = 0 if way == 0 else BLOCK + 512
        plow = 512 if way == 0 else EDGE
        phigh = 0 if way == 0 else EDGE + 512
        device = sequence_neighbour(1 if way == 0 else -1)
        return [
            remote(
                kv_ext.at[low : low + BLOCK], kv_ext.at[high : high + BLOCK],
                halo_send.at[way, 0], halo_recv.at[way, 0], device,
            ),
            remote(
                pool_ext.at[plow : plow + EDGE], pool_ext.at[phigh : phigh + EDGE],
                halo_send.at[way, 1], halo_recv.at[way, 1], device,
            ),
        ]

    reach = lax.shift_left(jnp.int32(1), x)
    scatter = Scatter(
        (far, near, far_in, near_in, kept), (far_send, far_recv, near_send, near_recv)
    )

    def block(i, carry):
        b = lax.rem(i + 1, 4)
        for h in range(2):
            attend(b, h, place, places, kv_ext, queries, sink_ref, features, log_ref)
        pool(b, place, places, reach, pool_ext, mix_ref, features)
        return carry

    def send(i, carry):
        b = lax.rem(i + 1, 4)
        scatter.compute(b, features, oa, ob)

        @pl.when(i > 0)
        def _():
            scatter.add(i)

        return carry

    def both(i, carry):
        block(i, carry)
        return send(i, carry)

    for t in outs:
        t.phase1_start()
    first(ins)
    levels(ins, 2)
    ring.forward()
    first(outs)
    levels(ins, 3)
    levels(outs, 2)
    levels(ins, 4)
    levels(outs, 3)
    ring.arrived()
    normalise(t_buf, gain_ref, normed)
    levels(ins, 5)
    for t in ins:
        t.arrived()
    project_keys(normed, wb, cos_ref, sin_ref, kv_ext)
    project_pool(normed, wb, pool_ext)
    for way in range(2):
        for copy in halo_copies(way):
            copy.start()
    project_queries(normed, wa, cos_ref, sin_ref, queries, 0)
    levels(outs, 4)
    project_queries(normed, wa, cos_ref, sin_ref, queries, 1)
    block(0, 0)
    levels(outs, 5)
    for t in outs:
        t.arrived()
    send(0, 0)
    lax.fori_loop(1, 2, both, 0)
    for way in range(2):
        for copy in halo_copies(way):
            copy.wait_recv()
    lax.fori_loop(2, 4, both, 0)
    scatter.add(0)

    def close(i, carry):
        b = lax.rem(i + 1, 4)
        scatter.finish(b, out_ref)
        scatter.drain(b)
        return carry

    lax.fori_loop(0, 4, close, 0)
    for t in ins + outs:
        t.drain()
    ring.drain()
    for way in range(2):
        for copy in halo_copies(way):
            copy.wait_send()


def whole_layer(tokens, weights, gain, mix, freq, sink):
    nz, ny, nc, nx = (lax.axis_size(a) for a in (AX_Z, AX_Y, AX_C, AX_X))
    rows, width = tokens.shape
    bf = jnp.bfloat16
    dma = pltpu.SemaphoreType.DMA
    vmem = pltpu.VMEM
    blocks = rows // BLOCK
    near_data = pl.BlockSpec(memory_space=pltpu.VMEM)
    return pl.pallas_call(
        layer_kernel,
        out_shape=[
            vmem((rows, width), bf),
            vmem((8, rows), jnp.float32),
        ],
        in_specs=[pl.BlockSpec(memory_space=pltpu.HBM)] * 9 + [near_data]
        + [pl.BlockSpec(memory_space=pltpu.SMEM)],
        out_specs=[near_data] * 2,
        scratch_shapes=[
            vmem((nx, rows, width), bf),
            vmem((nz, ny, nc, 16, 512), bf),
            vmem((nz, ny, nc, 16, 512), bf),
            vmem((nz, ny, nc, 16, 384), bf),
            vmem((nz, ny, nc, 16, 384), bf),
            vmem((1, nx * width), jnp.float32),
            vmem((1, 256, 256), bf),
            vmem((rows, 128), jnp.float32),
            vmem((rows, 128), jnp.float32),
            vmem((rows, nx * width), bf),
            vmem((2, blocks, 4 * BLOCK, 128), bf),
            vmem((rows + 2 * BLOCK, 256), bf),
            vmem((rows + 2 * EDGE, 256), bf),
            vmem((rows, 768), bf),
            vmem((blocks, BLOCK, 512), bf),
            vmem((blocks, 2, BLOCK, 512), bf),
            vmem((blocks, 2, BLOCK // 2, 512), bf),
            vmem((blocks, 2, BLOCK, 512), bf),
            vmem((blocks, BLOCK, 512), bf),
            dma((10,)), dma((2, 3)), dma((2, 3)), dma((2, 2)), dma((2, 2)),
            dma((blocks, 2)), dma((blocks, 2)), dma((blocks, 2, 2)), dma((blocks, 2, 2)),
        ]
        + torus_sems(ny, nz, 4) + torus_sems(nz, ny, 4) + torus_sems(ny, nz, 8) + torus_sems(nz, ny, 8),
        compiler_params=pltpu.CompilerParams(
            collective_id=0, has_side_effects=True, vmem_limit_bytes=56 * 1024 * 1024
        ),
    )(tokens, *weights, gain, mix, freq, sink)


def local(
    tokens,
    norm_gain,
    query_weight,
    key_weight,
    value_weight,
    pool_in_weight,
    pool_mix_weight,
    sink_logit,
    out_pool_weight,
    out_attn_weight,
):
    lane = np.arange(128)
    freq = (rope_base ** (-(lane % 16) / 16.0)).astype(np.float32)[None]
    mixed, log_weight = whole_layer(
        tokens,
        (query_weight, key_weight, value_weight, pool_in_weight, out_pool_weight.T, out_attn_weight.T),
        norm_gain[None],
        pool_mix_weight,
        jnp.asarray(freq),
        sink_logit,
    )
    return (mixed, log_weight)


def solution(mesh):
    finer = Mesh(mesh.devices.reshape(8, 8, 2, mesh.shape["tp"]), ("sp_0", "sp_1", "sp_2", "tp"))
    placed = (
        P(SP, "tp"),
        P(),
        P(SP, "tp"),
        P(SP, "tp"),
        P(SP, "tp"),
        P(SP, "tp"),
        P("tp", None, None),
        P("tp"),
        P("tp", SP),
        P("tp", SP),
    )
    return jax.shard_map(
        local, mesh=finer, in_specs=placed, out_specs=(P(SP, "tp"), P("tp", SP)), check_vma=False
    )
```
